512 devices in a mesh: sp: 16 (over y, x), tp: 32 (over z, core).
Axes of the slice: x: 4, y: 4, z: 16, core: 2. Of those that a mesh axis runs over, the one named last changes fastest.
Arguments:
- tokens: bfloat16 [8, 49152, 2048], P(None, ('sp', 'tp')), may hold values from -13 to 13
- in_gain: float32 [2048], replicated, may hold values from 0.1 to 1.9
- w_key: bfloat16 [2048, 512], P('tp'), may hold values from -0.125 to 0.125
- w_value: bfloat16 [2048, 512], P('tp'), may hold values from -0.125 to 0.125
- k_gain: float32 [128], replicated, may hold values from 0.1 to 1.9
- new_query: bfloat16 [8, 1024], replicated, may hold values from -6 to 6
- q_gain: float32 [128], replicated, may hold values from 0.1 to 1.9
- stick_bias: float32 [8], replicated, may hold values from -13 to -3
Outputs:
- key_cache: bfloat16 [32, 49152, 128], P('tp', 'sp')
- value_cache: bfloat16 [32, 49152, 128], P('tp', 'sp')
- read_out: float32 [32, 256], P('tp')
The draws below stay inside these ranges and needn't reach their ends.
All inputs are finite; a program needn't handle non-finite values.
Results may differ from the reference program's by a relative error of at most 0.005.
Values may be sent and summed in bfloat16 or wider, within the bound.
No kernel may reach another device: no remote copies, remote signals or barrier semaphores. Data moves between devices by JAX's collectives and lax.ppermute only.
A program may use at most 64 MiB of HBM per device.

```python
import jax
import jax.numpy as jnp
from jax import lax

D = 2048
HEADS = 8
KVH = 4
HD = 128
SEQS = 8
LENGTH = 49152


def draw_tokens(key, part):
    noise_key, common_key, level_key = jax.random.split(jax.random.fold_in(key, 11), 3)
    block_count = LENGTH // 32
    noise_part = jnp.clip(jax.random.normal(noise_key, (SEQS, LENGTH, D), jnp.float32), -5.0, 5.0)
    levels = jnp.exp(jax.random.uniform(level_key, (SEQS, block_count, 1), jnp.float32, -1.2, 0.9))
    common = jnp.clip(jax.random.normal(common_key, (SEQS, 1, D), jnp.float32), -3.0, 3.0)
    levels = jnp.repeat(levels, 32, axis=1)
    return (noise_part + levels * common).astype(jnp.bfloat16)


def draw_stick_bias(key, part):
    order_key, fast_key, slow_key = jax.random.split(jax.random.fold_in(key, 23), 3)
    chain = jnp.log(jnp.float32(LENGTH))
    slow_bias = -chain + jax.random.uniform(slow_key, (HEADS,), jnp.float32, -1.5, 0.0)
    fast_bias = jax.random.uniform(fast_key, (HEADS,), jnp.float32, -4.5, -3.5)
    ranking = jax.random.permutation(order_key, HEADS)
    is_fast = ranking < HEADS // 2
    return jnp.where(is_fast, fast_bias, slow_bias)


def steps_of(own_key, shape, pieces, least, high):
    loudness = 1.0
    for axis_at, parts in pieces:
        heights = jax.random.uniform(jax.random.fold_in(jax.random.fold_in(own_key, 6), axis_at), (parts,), jnp.float32, least / len(pieces), high / len(pieces))
        loudness = loudness * jnp.repeat(jnp.exp(heights), shape[axis_at] // parts).reshape((-1,) + (1,) * (len(shape) - 1 - axis_at))
    return loudness


def bell_draw(rng, dims, deviation, reach, pieces=(), dtype=jnp.bfloat16):
    loudness = steps_of(rng, dims, pieces, -0.22, 0.18) if pieces else 1.0
    result = jax.random.normal(rng, dims, jnp.float32) * deviation * loudness
    return jnp.minimum(jnp.maximum(result, -reach), reach).astype(dtype)


def setup_inputs(seed: int = 0) -> dict:
    streams_of = jax.random.split(jax.random.key(seed), 9)
    return {
        "tokens": draw_tokens(jax.random.fold_in(streams_of[8], 71), 0),
        "in_gain": jnp.clip(1.0 + 0.18 * jax.random.normal(streams_of[1], (D,), jnp.float32), 0.1, 1.9),
        "w_key": bell_draw(streams_of[2], (D, KVH * HD), D ** -0.5, 0.125, ((0, 32),)),
        "w_value": bell_draw(streams_of[3], (D, KVH * HD), D ** -0.5, 0.125, ((0, 32),)),
        "k_gain": jnp.clip(1.0 + 0.18 * jax.random.normal(streams_of[4], (HD,), jnp.float32), 0.1, 1.9),
        "new_query": bell_draw(streams_of[5], (SEQS, HEADS * HD), 1.0, 6.0),
        "q_gain": jnp.clip(1.0 + 0.18 * jax.random.normal(streams_of[6], (HD,), jnp.float32), 0.1, 1.9),
        "stick_bias": draw_stick_bias(jax.random.fold_in(streams_of[8], 71), 0),
    }


NORM_EPS = 1e-06

def root_norm(values, scaling):
    inverse = lax.rsqrt(lax.optimization_barrier(jnp.mean(values * values, axis=-1, keepdims=True)) + NORM_EPS)
    return values * inverse * scaling

def reference(tokens, in_gain, w_key, w_value, k_gain, new_query, q_gain, stick_bias):
    per_group = HEADS // KVH
    query_rows = root_norm(new_query.astype(jnp.float32).reshape(SEQS, KVH, per_group, HD), q_gain).astype(jnp.bfloat16)
    bias_rows = stick_bias.astype(jnp.float32).reshape(KVH, per_group)

    def per_sequence(inputs):
        seq_tokens, seq_query = inputs
        normed = root_norm(seq_tokens.astype(jnp.float32), in_gain).astype(jnp.bfloat16)
        key_raw = jnp.dot(normed, w_key, preferred_element_type=jnp.float32).reshape(LENGTH, KVH, HD)
        key_rows = root_norm(key_raw, k_gain).astype(jnp.bfloat16)
        value_rows = jnp.dot(normed, w_value, preferred_element_type=jnp.float32).astype(jnp.bfloat16).reshape(LENGTH, KVH, HD)
        scores = jnp.einsum('hqe,phe->hqp', seq_query.astype(jnp.float32), key_rows.astype(jnp.float32)) * HD ** (-0.5) + bias_rows[:, :, None]
        log_keep = jax.nn.log_sigmoid(-scores)
        log_after = lax.cumsum(log_keep, axis=2, reverse=True) - log_keep
        weights = jnp.exp(jax.nn.log_sigmoid(scores) + log_after).astype(jnp.bfloat16)
        read_rows = jnp.einsum('hqp,phe->hqe', weights.astype(jnp.float32), value_rows.astype(jnp.float32))
        return (key_rows.transpose(1, 0, 2), value_rows.transpose(1, 0, 2), read_rows.reshape(KVH, per_group * HD))
    key_all, value_all, read_all = lax.map(per_sequence, (tokens, query_rows))
    key_cache = key_all.transpose(1, 0, 2, 3).reshape(KVH * SEQS, LENGTH, HD)
    value_cache = value_all.transpose(1, 0, 2, 3).reshape(KVH * SEQS, LENGTH, HD)
    read_out = read_all.transpose(1, 0, 2).reshape(KVH * SEQS, per_group * HD)
    return (key_cache, value_cache, read_out)
```

```python
import functools

import jax
import jax.numpy as jnp
from jax import lax
from jax.experimental import pallas as pl
from jax.experimental.pallas import tpu as pltpu
from jax.sharding import Mesh
from jax.sharding import PartitionSpec as P

NORM_EPS = 1e-06
SP = ("y", "x")
EXTRA = 8
F32 = jnp.float32
BF16 = jnp.bfloat16


def root_norm(values, scaling):
    inverse = lax.rsqrt(jnp.mean(values * values, axis=-1, keepdims=True) + NORM_EPS)
    return values * inverse * scaling


def to_all(piece, axis):
    count = lax.axis_size(axis)
    return lax.all_to_all(
        jnp.broadcast_to(piece[None], (count, *piece.shape)), axis, 0, 0, tiled=True
    )


def gathered_rows(w_key, w_value):
    columns = lax.axis_size(SP)
    mine = lax.axis_index(SP)
    per = columns // 2
    rows = w_key.shape[0] // per
    at = (mine % per) * rows
    piece = jnp.where(
        mine < per,
        lax.dynamic_slice_in_dim(w_key, at, rows, 0),
        lax.dynamic_slice_in_dim(w_value, at, rows, 0),
    )
    along_z = to_all(piece, "z")
    return to_all(along_z, SP)


def high_low(values):
    high = values.astype(BF16)
    return high, (values - high.astype(F32)).astype(BF16)


def project_kernel(
    x_ref, own_ref, other_ref, query_ref, bias_ref, gain_ref, out_ref, wk_ref, wv_ref, sems
):
    core = lax.axis_index("c")
    pieces = own_ref.shape[0] // 2
    rows = own_ref.shape[2]
    seqs = query_ref.shape[0]
    heads = query_ref.shape[1]
    hd = gain_ref.shape[1]
    span = x_ref.shape[0] // seqs
    width = own_ref.shape[3]
    kv_heads = width // hd
    per_group = heads // kv_heads

    def copies(which):
        dst = (wk_ref, wv_ref)[which]
        out = []
        for t, (src, at) in enumerate(((own_ref, core), (other_ref, 1 - core))):
            for r in range(pieces):
                out.append(
                    pltpu.make_async_copy(
                        src.at[which * pieces + r],
                        dst.at[:, at, pl.ds(r * rows, rows), :],
                        sems.at[which, t, r],
                    )
                )
        return out

    key_copies, value_copies = copies(0), copies(1)
    for copy in key_copies + value_copies:
        copy.start()
    x = x_ref[...]
    model = x.shape[1]
    gain = gain_ref[...]
    wide = 2 * hd

    for copy in key_copies:
        copy.wait()
    for h in range(width // wide):
        w = wk_ref[:, :, :, h * wide : (h + 1) * wide].reshape(model, wide)
        raw = jnp.dot(x, w, preferred_element_type=F32)
        for k in range(2):
            g = 2 * h + k
            head = root_norm(raw[:, k * hd : (k + 1) * hd], gain).astype(BF16)
            for i in range(seqs):
                out_ref[g * seqs + i, 0:span, :] = head[i * span : (i + 1) * span]
    for copy in value_copies:
        copy.wait()
    for h in range(width // wide):
        w = wv_ref[:, :, :, h * wide : (h + 1) * wide].reshape(model, wide)
        raw = jnp.dot(x, w, preferred_element_type=F32).astype(BF16)
        for k in range(2):
            g = 2 * h + k
            for i in range(seqs):
                out_ref[g * seqs + i, span : 2 * span, :] = raw[
                    i * span : (i + 1) * span, k * hd : (k + 1) * hd
                ]

    scores = []
    for i in range(seqs):
        total = jnp.zeros((heads, span), F32)
        for g in range(kv_heads):
            total += lax.dot_general(
                query_ref[i, :, g * hd : (g + 1) * hd],
                out_ref[g * seqs + i, 0:span, :],
                (((1,), (1,)), ((), ())),
                preferred_element_type=F32,
            )
        scores.append(total * (hd**-0.5) + bias_ref[...])
    scores = jnp.concatenate(scores, axis=0)
    log_keep = -(jnp.maximum(scores, 0.0) + jnp.log1p(jnp.exp(-jnp.abs(scores))))
    first = lax.broadcasted_iota(jnp.int32, (span, span), 0)
    second = lax.broadcasted_iota(jnp.int32, (span, span), 1)
    later = (first > second).astype(BF16)
    after = jnp.zeros(scores.shape, F32)
    rest = log_keep
    for _ in range(3):
        part = rest.astype(BF16)
        rest = rest - part.astype(F32)
        after += jnp.dot(part, later, preferred_element_type=F32)
    weight_high, weight_low = high_low(jnp.exp(scores + log_keep + after))
    total = jnp.sum(log_keep, axis=1, keepdims=True)
    total_high, total_low = high_low(total)
    put = lax.broadcasted_iota(jnp.int32, (EXTRA, 4 * heads), 0)
    take = lax.broadcasted_iota(jnp.int32, (EXTRA, 4 * heads), 1)
    for i in range(seqs):
        at = slice(i * heads, (i + 1) * heads)
        for g in range(kv_heads):
            values = out_ref[g * seqs + i, span : 2 * span, :]
            read = jnp.dot(weight_high[at], values, preferred_element_type=F32) + jnp.dot(
                weight_low[at], values, preferred_element_type=F32
            )
            read_high, read_low = high_low(read)
            stacked = jnp.concatenate(
                [
                    read_high.astype(F32),
                    read_low.astype(F32),
                    jnp.broadcast_to(total_high[at].astype(F32), read.shape),
                    jnp.broadcast_to(total_low[at].astype(F32), read.shape),
                ],
                axis=0,
            ).astype(BF16)
            pick = (
                take == (put // per_group) * heads + g * per_group + put % per_group
            ).astype(BF16)
            out_ref[g * seqs + i, 2 * span :, :] = jnp.dot(
                pick, stacked, preferred_element_type=F32
            ).astype(BF16)


def project(x, own, other, query, bias, gain):
    seqs, heads, width = query.shape
    hd = gain.shape[1]
    span = x.shape[0] // seqs
    blocks = (width // hd) * seqs
    pieces, zs, rows, _ = own.shape
    half = pieces // 2
    scratch = pltpu.VMEM((zs, 2, half * rows, width), BF16)
    vmem = pl.BlockSpec(memory_space=pltpu.VMEM)
    hbm = pl.BlockSpec(memory_space=pl.ANY)
    return pl.pallas_call(
        project_kernel,
        out_shape=jax.ShapeDtypeStruct((blocks, 2 * span + EXTRA, hd), BF16),
        in_specs=[vmem, hbm, hbm, vmem, vmem, vmem],
        out_specs=vmem,
        scratch_shapes=[scratch, scratch, pltpu.SemaphoreType.DMA((2, 2, half))],
        compiler_params=pltpu.CompilerParams(vmem_limit_bytes=48 * 1024 * 1024),
        name="project",
    )(x, own, other, query, bias, gain)


def join_first_kernel(rows_ref, out_ref):
    count = rows_ref.shape[0]
    shape = (2, rows_ref.shape[2])
    read, log_later = jnp.zeros(shape, F32), jnp.zeros(shape, F32)
    for n in reversed(range(count)):
        rows = rows_ref[n].astype(F32)
        read += jnp.exp(log_later) * (rows[0:2] + rows[2:4])
        log_later += rows[4:6] + rows[6:8]
    out_ref[0:2] = read
    out_ref[2:4] = log_later


def join_last_kernel(rows_ref, out_ref):
    count = rows_ref.shape[0]
    shape = (2, rows_ref.shape[2])
    read, log_later = jnp.zeros(shape, F32), jnp.zeros(shape, F32)
    for n in reversed(range(count)):
        read += jnp.exp(log_later) * rows_ref[n, 0:2]
        log_later += rows_ref[n, 2:4]
    out_ref[...] = read


def join_first(received):
    count, rows, hd = received.shape
    return pl.pallas_call(
        join_first_kernel,
        grid=(1,),
        out_shape=jax.ShapeDtypeStruct((4, hd), F32),
        in_specs=[pl.BlockSpec((count, EXTRA, hd), lambda i: (0, rows // EXTRA - 1, 0))],
        out_specs=pl.BlockSpec((4, hd), lambda i: (0, 0)),
        name="join_first",
    )(received)


def join_last(pieces):
    return pl.pallas_call(
        join_last_kernel,
        out_shape=jax.ShapeDtypeStruct((2, pieces.shape[2]), F32),
        name="join_last",
    )(pieces)


def shards(tokens, in_gain, w_key, w_value, k_gain, new_query, q_gain, stick_bias):
    seq_count, tok_seq, model_width = tokens.shape
    head_dim = k_gain.shape[0]
    heads = stick_bias.shape[0]
    kv_heads = w_key.shape[1] // head_dim
    per_group = heads // kv_heads
    seqs = seq_count // 2
    core = lax.axis_index("c")

    own = gathered_rows(w_key, w_value)
    other = lax.ppermute(own, "c", [(0, 1), (1, 0)])

    paired = tokens.reshape(seqs, 2, tok_seq, model_width)
    kept = lax.dynamic_index_in_dim(paired, core, 1, False)
    sent = lax.dynamic_index_in_dim(paired, 1 - core, 1, False)
    came = lax.ppermute(sent, "c", [(0, 1), (1, 0)])
    low = jnp.where(core == 0, kept, came)
    high = jnp.where(core == 0, came, kept)
    span_tokens = jnp.stack([low, high], axis=1).reshape(seqs * 2 * tok_seq, model_width)
    normed = root_norm(span_tokens.astype(F32), in_gain).astype(BF16)

    query = root_norm(
        new_query.astype(F32).reshape(seqs, 2, heads, head_dim)[:, 0], q_gain
    )
    query_odd = root_norm(
        new_query.astype(F32).reshape(seqs, 2, heads, head_dim)[:, 1], q_gain
    )
    query = jnp.where(core == 0, query, query_odd).astype(BF16)
    of_group = jnp.arange(heads)[:, None] // per_group == jnp.arange(kv_heads)[None, :]
    query = jnp.where(of_group[None, :, :, None], query[:, :, None, :], 0).reshape(
        seqs, heads, kv_heads * head_dim
    )

    out = project(
        normed, own, other, query, stick_bias.reshape(heads, 1), k_gain.reshape(1, head_dim)
    )
    received = lax.all_to_all(out, "z", 0, 0, tiled=True)
    span = 2 * tok_seq
    joined = join_first(received)
    everything = to_all(joined, SP)
    read = join_last(everything)
    positions = received.shape[0] * span
    key_cache = received[:, :span].reshape(1, positions, head_dim)
    value_cache = received[:, span : 2 * span].reshape(1, positions, head_dim)
    return (key_cache, value_cache, read.reshape(1, per_group * head_dim))


def solution(mesh):
    grid = Mesh(mesh.devices.reshape(4, 4, 16, 2), ("y", "x", "z", "c"))
    tp = ("z", "c")
    return jax.shard_map(
        shards,
        mesh=grid,
        in_specs=(
            P(None, ("y", "x", "z", "c"), None),
            P(),
            P(tp, None),
            P(tp, None),
            P(),
            P(),
            P(),
            P(),
        ),
        out_specs=(P(tp, SP, None), P(tp, SP, None), P(tp, None)),
        check_vma=False,
    )
```

```python
import jax
import jax.numpy as jnp
from jax import lax
from jax.experimental import pallas as pl
from jax.experimental.pallas import tpu as pltpu
from jax.sharding import Mesh
from jax.sharding import PartitionSpec as P

NORM_EPS = 1e-06
SP = ("y", "x")
EXTRA = 8
F32 = jnp.float32
BF16 = jnp.bfloat16


def root_norm(values, scaling):
    inverse = lax.rsqrt(jnp.mean(values * values, axis=-1, keepdims=True) + NORM_EPS)
    return values * inverse * scaling


def to_all(piece, axis):
    count = lax.axis_size(axis)
    return lax.all_to_all(
        jnp.broadcast_to(piece[None], (count, *piece.shape)), axis, 0, 0, tiled=True
    )


def along_z(w_key, w_value):
    columns = lax.axis_size(SP)
    mine = lax.axis_index(SP)
    per = columns // 2
    rows = w_key.shape[0] // per
    at = (mine % per) * rows
    piece = jnp.where(
        mine < per,
        lax.dynamic_slice_in_dim(w_key, at, rows, 0),
        lax.dynamic_slice_in_dim(w_value, at, rows, 0),
    )
    return to_all(piece, "z")


def norm_kernel(tokens_ref, gain_ref, kept_ref, sent_ref):
    core = lax.axis_index("c")
    gain = gain_ref[...]
    kept_ref[0] = root_norm(tokens_ref[core].astype(F32), gain).astype(BF16)
    sent_ref[0] = root_norm(tokens_ref[1 - core].astype(F32), gain).astype(BF16)


def norm_halves(tokens, in_gain):
    seq_count, length, model = tokens.shape
    half = jax.ShapeDtypeStruct((seq_count // 2, length, model), BF16)
    block = pl.BlockSpec((1, length, model), lambda i: (i, 0, 0))
    return pl.pallas_call(
        norm_kernel,
        grid=(seq_count // 2,),
        out_shape=(half, half),
        in_specs=[
            pl.BlockSpec((2, length, model), lambda i: (i, 0, 0)),
            pl.BlockSpec((1, model), lambda i: (0, 0)),
        ],
        out_specs=(block, block),
        compiler_params=vmem(16),
        name="norm_halves",
    )(tokens, in_gain.reshape(1, model))


def spread_kernel(piece_ref, out_ref):
    piece = piece_ref[...]
    for n in range(out_ref.shape[0]):
        out_ref[n] = piece


def spread(piece, count):
    return pl.pallas_call(
        spread_kernel,
        out_shape=pltpu.VMEM((count, *piece.shape), piece.dtype),
        compiler_params=vmem(8),
        name="spread",
    )(*on_chip(piece))


def vmem(mib):
    return pltpu.CompilerParams(vmem_limit_bytes=mib * 1024 * 1024)


def on_chip(*arrays):
    return tuple(pltpu.with_memory_space_constraint(a, pltpu.VMEM) for a in arrays)


def high_low(values):
    high = values.astype(BF16)
    return high, (values - high.astype(F32)).astype(BF16)


def arrange_kernel(kept_ref, came_ref, query_ref, gain_ref, x_ref, grouped_ref):
    core = lax.axis_index("c")
    seqs, length, model = kept_ref.shape
    hd = gain_ref.shape[1]
    heads = query_ref.shape[1] // hd
    kv_heads = grouped_ref.shape[2] // hd
    zs = lax.axis_size("z")
    held = model // zs // 2
    rows = hd // zs
    pieces = held // rows
    wide = 2 * hd
    kept = kept_ref[...].reshape(seqs * length, model)
    came = came_ref[...].reshape(seqs * length, model)
    source = lax.broadcasted_iota(jnp.int32, (model, wide), 0)
    column = lax.broadcasted_iota(jnp.int32, (model, wide), 1)
    inside = column % hd
    target = (inside // rows) * (2 * held) + (column // hd) * rows + inside % rows
    offset = source - target
    for half in range(2):
        for r in range(0, pieces, 2):
            pick = (offset == half * held + r * rows).astype(BF16)
            at = slice(r * hd, r * hd + wide)
            x_ref[half, core, :, at] = jnp.dot(kept, pick, preferred_element_type=F32).astype(BF16)
            x_ref[half, 1 - core, :, at] = jnp.dot(
                came, pick, preferred_element_type=F32
            ).astype(BF16)

    query = query_ref[...].astype(F32)
    row = lax.broadcasted_iota(jnp.int32, (heads, hd), 0)
    per_group = heads // kv_heads
    for i in range(seqs):
        mine = jnp.where(core == 0, query[2 * i : 2 * i + 1], query[2 * i + 1 : 2 * i + 2])
        for g in range(kv_heads):
            block = jnp.zeros((heads, hd), F32)
            for j in range(g * per_group, (g + 1) * per_group):
                head = root_norm(mine[:, j * hd : (j + 1) * hd], gain_ref[...])
                block = jnp.where(row == j, head, block)
            grouped_ref[i, :, g * hd : (g + 1) * hd] = block.astype(BF16)


def arrange(kept, came, new_query, q_gain, kv_heads):
    seqs, length, model = kept.shape
    hd = q_gain.shape[0]
    heads = new_query.shape[1] // hd
    return pl.pallas_call(
        arrange_kernel,
        out_shape=(
            pltpu.VMEM((2, 2, seqs * length, model // 2), BF16),
            pltpu.VMEM((seqs, heads, kv_heads * hd), BF16),
        ),
        compiler_params=vmem(32),
        name="arrange",
    )(kept, came, new_query, q_gain.reshape(1, hd))


def partial_kernel(x_ref, rows_ref, out_ref):
    core = lax.axis_index("c")
    x = x_ref[core]
    for which in range(rows_ref.shape[0]):
        out_ref[which] = jnp.dot(x, rows_ref[which], preferred_element_type=F32)


def partial_product(x, own):
    return pl.pallas_call(
        partial_kernel,
        out_shape=pltpu.VMEM((2, x.shape[1], own.shape[2]), F32),
        compiler_params=vmem(16),
        name="partial",
    )(*on_chip(x, own))


def finish_kernel(x_ref, rows_ref, begun_ref, query_ref, bias_ref, gain_ref, key_ref, value_ref):
    core = lax.axis_index("c")
    seqs, heads, width = query_ref.shape
    hd = gain_ref.shape[1]
    length = x_ref.shape[1] // (2 * seqs)
    span = 2 * length
    kv_heads = width // hd
    per_group = heads // kv_heads
    wide = 2 * hd
    x = x_ref[1 - core]
    gain = gain_ref[...]

    def place(ref, g, head):
        for n in range(2 * seqs):
            h, i = divmod(n, seqs)
            ref[g * seqs + i, h * length : (h + 1) * length, :] = head[n * length : (n + 1) * length]

    for start in range(0, width, wide):
        at = slice(start, start + wide)
        raw = begun_ref[0, :, at] + jnp.dot(x, rows_ref[0, :, at], preferred_element_type=F32)
        for k in range(2):
            head = root_norm(raw[:, k * hd : (k + 1) * hd], gain).astype(BF16)
            place(key_ref, start // hd + k, head)

    row = lax.broadcasted_iota(jnp.int32, (heads, 1), 0)
    bias = jnp.zeros((heads, 1), F32)
    for j in range(heads):
        bias = jnp.where(row == j, bias_ref[j], bias)
    scores = []
    for i in range(seqs):
        total = jnp.zeros((heads, span), F32)
        for g in range(kv_heads):
            total += lax.dot_general(
                query_ref[i, :, g * hd : (g + 1) * hd],
                key_ref[g * seqs + i, 0:span, :],
                (((1,), (1,)), ((), ())),
                preferred_element_type=F32,
            )
        scores.append(total * (hd**-0.5) + bias)
    scores = jnp.concatenate(scores, axis=0)
    log_keep = -(jnp.maximum(scores, 0.0) + jnp.log1p(jnp.exp(-jnp.abs(scores))))
    first = lax.broadcasted_iota(jnp.int32, (span, span), 0)
    second = lax.broadcasted_iota(jnp.int32, (span, span), 1)
    later = (first > second).astype(BF16)
    after = jnp.zeros(scores.shape, F32)
    rest = log_keep
    for _ in range(3):
        part = rest.astype(BF16)
        rest = rest - part.astype(F32)
        after += jnp.dot(part, later, preferred_element_type=F32)
    weight_high, weight_low = high_low(jnp.exp(scores + log_keep + after))
    total_high, total_low = high_low(jnp.sum(log_keep, axis=1, keepdims=True))

    for start in range(0, width, wide):
        at = slice(start, start + wide)
        raw = begun_ref[1, :, at] + jnp.dot(x, rows_ref[1, :, at], preferred_element_type=F32)
        for k in range(2):
            place(value_ref, start // hd + k, raw[:, k * hd : (k + 1) * hd].astype(BF16))

    put = lax.broadcasted_iota(jnp.int32, (EXTRA, 4 * heads), 0)
    take = lax.broadcasted_iota(jnp.int32, (EXTRA, 4 * heads), 1)
    for i in range(seqs):
        at = slice(i * heads, (i + 1) * heads)
        for g in range(kv_heads):
            values = value_ref[g * seqs + i]
            read = jnp.dot(weight_high[at], values, preferred_element_type=F32) + jnp.dot(
                weight_low[at], values, preferred_element_type=F32
            )
            read_high, read_low = high_low(read)
            stacked = jnp.concatenate(
                [
                    read_high.astype(F32),
                    read_low.astype(F32),
                    jnp.broadcast_to(total_high[at].astype(F32), read.shape),
                    jnp.broadcast_to(total_low[at].astype(F32), read.shape),
                ],
                axis=0,
            ).astype(BF16)
            pick = (
                take == (put // per_group) * heads + g * per_group + put % per_group
            ).astype(BF16)
            key_ref[g * seqs + i, span:, :] = jnp.dot(
                pick, stacked, preferred_element_type=F32
            ).astype(BF16)


def finish(x, other, begun, query, bias, gain):
    seqs, _, width = query.shape
    hd = gain.shape[0]
    span = x.shape[1] // seqs
    blocks = (width // hd) * seqs
    here = pl.BlockSpec(memory_space=pltpu.VMEM)
    return pl.pallas_call(
        finish_kernel,
        out_shape=(
            pltpu.VMEM((blocks, span + EXTRA, hd), BF16),
            pltpu.VMEM((blocks, span, hd), BF16),
        ),
        in_specs=[here, here, here, here, pl.BlockSpec(memory_space=pltpu.SMEM), here],
        compiler_params=vmem(24),
        name="finish",
    )(*on_chip(x, other, begun, query), bias, gain.reshape(1, hd))


def join_first_kernel(rows_ref, out_ref):
    count = rows_ref.shape[0]
    shape = (2, rows_ref.shape[2])
    read, log_later = jnp.zeros(shape, F32), jnp.zeros(shape, F32)
    for n in reversed(range(count)):
        rows = rows_ref[n, rows_ref.shape[1] - EXTRA :].astype(F32)
        read += jnp.exp(log_later) * (rows[0:2] + rows[2:4])
        log_later += rows[4:6] + rows[6:8]
    out_ref[0:2] = read
    out_ref[2:4] = log_later


def join_last_kernel(rows_ref, out_ref):
    count = rows_ref.shape[0]
    shape = (2, rows_ref.shape[2])
    read, log_later = jnp.zeros(shape, F32), jnp.zeros(shape, F32)
    for n in reversed(range(count)):
        read += jnp.exp(log_later) * rows_ref[n, 0:2]
        log_later += rows_ref[n, 2:4]
    out_ref[...] = read


def join_first(received):
    return pl.pallas_call(
        join_first_kernel,
        out_shape=pltpu.VMEM((4, received.shape[2]), F32),
        compiler_params=vmem(8),
        name="join_first",
    )(*on_chip(received))


def join_last(pieces):
    return pl.pallas_call(
        join_last_kernel,
        out_shape=jax.ShapeDtypeStruct((2, pieces.shape[2]), F32),
        compiler_params=vmem(4),
        name="join_last",
    )(*on_chip(pieces))


def shards(tokens, in_gain, w_key, w_value, k_gain, new_query, q_gain, stick_bias):
    seq_count, tok_seq, model_width = tokens.shape
    head_dim = k_gain.shape[0]
    heads = stick_bias.shape[0]
    kv_heads = w_key.shape[1] // head_dim
    per_group = heads // kv_heads
    pieces = along_z(w_key, w_value)
    kept, sent = norm_halves(tokens, in_gain)
    own = lax.all_to_all(spread(pieces, lax.axis_size(SP)), SP, 0, 0, tiled=True)
    own = own.reshape(2, model_width // 2, w_key.shape[1])
    came = lax.ppermute(sent, "c", [(0, 1), (1, 0)])
    x, query = arrange(kept, came, new_query, q_gain, kv_heads)
    x = x.reshape(2, seq_count * tok_seq, model_width // 2)
    other = lax.ppermute(own, "c", [(0, 1), (1, 0)])
    begun = partial_product(x, own)
    keys, values = finish(x, other, begun, query, stick_bias, k_gain)
    got_keys = lax.all_to_all(keys, "z", 0, 0, tiled=True)
    got_values = lax.all_to_all(values, "z", 0, 0, tiled=True)
    joined = join_first(got_keys)
    everything = lax.all_gather(joined, SP)
    read = join_last(everything)
    span = 2 * tok_seq
    positions = got_keys.shape[0] * span
    key_cache = got_keys[:, :span].reshape(1, positions, head_dim)
    value_cache = got_values.reshape(1, positions, head_dim)
    return (key_cache, value_cache, read.reshape(1, per_group * head_dim))


def solution(mesh):
    grid = Mesh(mesh.devices.reshape(4, 4, 16, 2), ("y", "x", "z", "c"))
    tp = ("z", "c")
    return jax.shard_map(
        shards,
        mesh=grid,
        in_specs=(
            P(None, ("y", "x", "z", "c"), None),
            P(),
            P(tp, None),
            P(tp, None),
            P(),
            P(),
            P(),
            P(),
        ),
        out_specs=(P(tp, SP, None), P(tp, SP, None), P(tp, None)),
        check_vma=False,
    )
```

```python
import functools

import jax
import jax.numpy as jnp
from jax import lax
from jax.experimental import pallas as pl
from jax.experimental.pallas import tpu as pltpu
from jax.sharding import Mesh
from jax.sharding import PartitionSpec as P

NORM_EPS = 1e-06
SP = ("y", "x")
EXTRA = 8
F32 = jnp.float32
BF16 = jnp.bfloat16


def root_norm(values, scaling):
    inverse = lax.rsqrt(jnp.mean(values * values, axis=-1, keepdims=True) + NORM_EPS)
    return values * inverse * scaling


def to_all(piece, axis):
    count = lax.axis_size(axis)
    return lax.all_to_all(
        jnp.broadcast_to(piece[None], (count, *piece.shape)), axis, 0, 0, tiled=True
    )


def along_z(w_key, w_value):
    rows = w_key.shape[0] // lax.axis_size("x")
    width = w_key.shape[1] // lax.axis_size("y")
    at = (lax.axis_index("x") * rows, lax.axis_index("y") * width)
    parts = [lax.dynamic_slice(w, at, (rows, width)) for w in (w_key, w_value)]
    return to_all(jnp.stack(parts), "z")


def norm_kernel(tokens_ref, gain_ref, kept_ref, sent_ref):
    core = lax.axis_index("c")
    gain = gain_ref[...]
    kept_ref[0] = root_norm(tokens_ref[core].astype(F32), gain).astype(BF16)
    sent_ref[0] = root_norm(tokens_ref[1 - core].astype(F32), gain).astype(BF16)


def norm_halves(tokens, in_gain):
    seq_count, length, model = tokens.shape
    half = pltpu.HBM((seq_count // 2, length, model), BF16)
    block = pl.BlockSpec((1, length, model), lambda i: (i, 0, 0))
    return pl.pallas_call(
        norm_kernel,
        grid=(seq_count // 2,),
        out_shape=(half, half),
        in_specs=[
            pl.BlockSpec((2, length, model), lambda i: (i, 0, 0)),
            pl.BlockSpec((1, model), lambda i: (0, 0)),
        ],
        out_specs=(block, block),
        compiler_params=vmem(16),
        name="norm_halves",
    )(*off_chip(tokens, in_gain.reshape(1, model)))


def spread_kernel(pieces_ref, early_ref, late_ref):
    zs = pieces_ref.shape[0]
    early = early_ref.shape[1] - zs
    for n in range(early_ref.shape[0]):
        early_ref[n, :zs] = pieces_ref[:, 0]
        early_ref[n, zs:] = pieces_ref[:early, 1]
    late_ref[...] = pieces_ref[early:, 1]


def spread(pieces, count):
    zs, _, rows, width = pieces.shape
    early = zs // 8
    return pl.pallas_call(
        spread_kernel,
        out_shape=(
            jax.ShapeDtypeStruct((count, zs + early, rows, width), pieces.dtype),
            jax.ShapeDtypeStruct((zs - early, rows, width), pieces.dtype),
        ),
        compiler_params=vmem(8),
        name="spread",
    )(*on_chip(pieces))


def vmem(mib):
    return pltpu.CompilerParams(vmem_limit_bytes=mib * 1024 * 1024)


def on_chip(*arrays):
    return tuple(pltpu.with_memory_space_constraint(a, pltpu.VMEM) for a in arrays)


def off_chip(*arrays):
    return tuple(pltpu.with_memory_space_constraint(a, pltpu.HBM) for a in arrays)


def high_low(values):
    high = values.astype(BF16)
    return high, (values - high.astype(F32)).astype(BF16)


def arrange_kernel(
    kept_hbm, came_hbm, query_ref, gain_ref, x_ref, grouped_ref, kept_ref, came_ref, sems
):
    core = lax.axis_index("c")
    loads = [
        pltpu.make_async_copy(kept_hbm, kept_ref, sems.at[0]),
        pltpu.make_async_copy(came_hbm, came_ref, sems.at[1]),
    ]
    for load in loads:
        load.start()
    seqs, length, model = kept_ref.shape
    hd = gain_ref.shape[1]
    heads = query_ref.shape[1] // hd
    kv_heads = grouped_ref.shape[2] // hd
    zs, xs = lax.axis_size("z"), lax.axis_size("x")
    held = model // zs // 2
    rows = held // xs
    part = hd // rows
    deep = part * 2 * held
    source = lax.broadcasted_iota(jnp.int32, (deep, 2 * hd), 0)
    column = lax.broadcasted_iota(jnp.int32, (deep, 2 * hd), 1)
    inside = column % hd
    offset = source - (inside // rows) * (2 * held) - inside % rows - (column // hd) * rows

    query = query_ref[...].astype(F32)
    row = lax.broadcasted_iota(jnp.int32, (heads, hd), 0)
    per_group = heads // kv_heads
    for i in range(seqs):
        mine = jnp.where(core == 0, query[2 * i : 2 * i + 1], query[2 * i + 1 : 2 * i + 2])
        for g in range(kv_heads):
            block = jnp.zeros((heads, hd), F32)
            for j in range(g * per_group, (g + 1) * per_group):
                head = root_norm(mine[:, j * hd : (j + 1) * hd], gain_ref[...])
                block = jnp.where(row == j, head, block)
            grouped_ref[i, :, g * hd : (g + 1) * hd] = block.astype(BF16)
    for load in loads:
        load.wait()
    kept = kept_ref[...].reshape(seqs * length, model)
    came = came_ref[...].reshape(seqs * length, model)
    for half in range(2):
        for r in range(0, xs, 2):
            pick = (offset == half * held + r * rows).astype(BF16)
            for n in range(zs // part):
                for values, at in ((kept, core), (came, 1 - core)):
                    moved = jnp.dot(
                        values[:, n * deep : (n + 1) * deep], pick, preferred_element_type=F32
                    ).astype(BF16)
                    for k in range(2):
                        start = (r + k) * zs * rows + n * hd
                        x_ref[half, at, :, start : start + hd] = moved[:, k * hd : (k + 1) * hd]


def arrange(kept, came, new_query, q_gain, kv_heads):
    seqs, length, model = kept.shape
    hd = q_gain.shape[0]
    heads = new_query.shape[1] // hd
    return pl.pallas_call(
        arrange_kernel,
        out_shape=(
            pltpu.VMEM((2, 2, seqs * length, model // 2), BF16),
            pltpu.VMEM((seqs, heads, kv_heads * hd), BF16),
        ),
        in_specs=[pl.BlockSpec(memory_space=pl.ANY)] * 2
        + [pl.BlockSpec(memory_space=pltpu.VMEM)] * 2,
        scratch_shapes=[
            pltpu.VMEM(kept.shape, BF16),
            pltpu.VMEM(kept.shape, BF16),
            pltpu.SemaphoreType.DMA((2,)),
        ],
        compiler_params=vmem(32),
        name="arrange",
    )(*off_chip(kept), came, new_query, q_gain.reshape(1, hd))


def two_heads(refs, head):
    columns = []
    for g in (head, head + 1):
        blocks = [ref[g, n, first:last] for n in range(refs[0][0].shape[1]) for ref, first, last in refs]
        columns.append(jnp.concatenate(blocks, axis=0))
    return jnp.concatenate(columns, axis=1)


def key_part(early_ref, held):
    return ((early_ref, 0, held),)


def value_parts(early_ref, late_ref, held):
    first = held if early_ref.shape[2] > held else 0
    return ((early_ref, first, early_ref.shape[2]), (late_ref, 0, late_ref.shape[2]))


def partial_kernel(*refs):
    x_ref, *rows_refs, out_ref = refs
    x = x_ref[lax.axis_index("c")]
    heads, count, _, hd = rows_refs[0].shape
    held = x.shape[1] // count
    parts = key_part(*rows_refs, held) if len(rows_refs) == 1 else value_parts(*rows_refs, held)
    for g in range(0, heads, 2):
        out_ref[:, g * hd : (g + 2) * hd] = jnp.dot(
            x, two_heads(parts, g), preferred_element_type=F32
        )


def partial_product(x, rows):
    width = rows[0].shape[0] * rows[0].shape[-1]
    return pl.pallas_call(
        partial_kernel,
        out_shape=pltpu.VMEM((x.shape[1], width), F32),
        compiler_params=vmem(16),
        name="partial",
    )(*on_chip(x), *rows)


def place(ref, seqs, length, g, head):
    for n in range(2 * seqs):
        h, i = divmod(n, seqs)
        ref[g * seqs + i, h * length : (h + 1) * length, :] = head[n * length : (n + 1) * length]


def keys_kernel(x_ref, rows_ref, begun_ref, gain_ref, key_ref, rest_ref):
    x = x_ref[1 - lax.axis_index("c")]
    gain = gain_ref[...]
    kv_heads, hd = rows_ref.shape[0], gain.shape[1]
    held = x.shape[1] // rows_ref.shape[1]
    seqs = key_ref.shape[0] // kv_heads
    for g in range(0, kv_heads, 2):
        raw = begun_ref[:, g * hd : (g + 2) * hd] + jnp.dot(
            x, two_heads(key_part(rows_ref, held), g), preferred_element_type=F32
        )
        for k in range(2):
            head = root_norm(raw[:, k * hd : (k + 1) * hd], gain).astype(BF16)
            place(key_ref, seqs, key_ref.shape[1] // 2, g + k, head)
    rest_ref[...] = rows_ref[:, :, held:]


def make_keys(x, other, begun, gain, seqs):
    kv_heads, parts, rows, hd = other.shape
    rest = rows - x.shape[2] // parts
    return pl.pallas_call(
        keys_kernel,
        out_shape=(
            pltpu.HBM((kv_heads * seqs, x.shape[1] // seqs, hd), BF16),
            pltpu.HBM((kv_heads, parts, rest, hd), BF16),
        ),
        compiler_params=vmem(16),
        name="make_keys",
    )(*on_chip(x, other, begun), gain.reshape(1, hd))


def values_kernel(x_ref, early_ref, late_ref, begun_ref, key_ref, query_ref, bias_ref, value_ref):
    core = lax.axis_index("c")
    seqs, heads, width = query_ref.shape
    hd = key_ref.shape[2]
    span = key_ref.shape[1]
    kv_heads = width // hd
    per_group = heads // kv_heads
    x = x_ref[1 - core]
    held = x.shape[1] // early_ref.shape[1]

    row = lax.broadcasted_iota(jnp.int32, (heads, 1), 0)
    bias = jnp.zeros((heads, 1), F32)
    for j in range(heads):
        bias = jnp.where(row == j, bias_ref[j], bias)
    scores = []
    for i in range(seqs):
        total = jnp.zeros((heads, span), F32)
        for g in range(kv_heads):
            total += lax.dot_general(
                query_ref[i, :, g * hd : (g + 1) * hd],
                key_ref[g * seqs + i],
                (((1,), (1,)), ((), ())),
                preferred_element_type=F32,
            )
        scores.append(total * (hd**-0.5) + bias)
    scores = jnp.concatenate(scores, axis=0)
    log_keep = -(jnp.maximum(scores, 0.0) + jnp.log1p(jnp.exp(-jnp.abs(scores))))
    first = lax.broadcasted_iota(jnp.int32, (span, span), 0)
    second = lax.broadcasted_iota(jnp.int32, (span, span), 1)
    later = (first > second).astype(BF16)
    after = jnp.zeros(scores.shape, F32)
    rest = log_keep
    for _ in range(3):
        part = rest.astype(BF16)
        rest = rest - part.astype(F32)
        after += jnp.dot(part, later, preferred_element_type=F32)
    weight_high, weight_low = high_low(jnp.exp(scores + log_keep + after))
    total_high, total_low = high_low(jnp.sum(log_keep, axis=1, keepdims=True))

    for g in range(0, kv_heads, 2):
        raw = begun_ref[:, g * hd : (g + 2) * hd] + jnp.dot(
            x, two_heads(value_parts(early_ref, late_ref, held), g), preferred_element_type=F32
        )
        for k in range(2):
            place(value_ref, seqs, span // 2, g + k, raw[:, k * hd : (k + 1) * hd].astype(BF16))

    put = lax.broadcasted_iota(jnp.int32, (EXTRA, 4 * heads), 0)
    take = lax.broadcasted_iota(jnp.int32, (EXTRA, 4 * heads), 1)
    for i in range(seqs):
        at = slice(i * heads, (i + 1) * heads)
        for g in range(kv_heads):
            values = value_ref[g * seqs + i, 0:span]
            read = jnp.dot(weight_high[at], values, preferred_element_type=F32) + jnp.dot(
                weight_low[at], values, preferred_element_type=F32
            )
            read_high, read_low = high_low(read)
            stacked = jnp.concatenate(
                [
                    read_high.astype(F32),
                    read_low.astype(F32),
                    jnp.broadcast_to(total_high[at].astype(F32), read.shape),
                    jnp.broadcast_to(total_low[at].astype(F32), read.shape),
                ],
                axis=0,
            ).astype(BF16)
            pick = (
                take == (put // per_group) * heads + g * per_group + put % per_group
            ).astype(BF16)
            value_ref[g * seqs + i, span:, :] = jnp.dot(
                pick, stacked, preferred_element_type=F32
            ).astype(BF16)


def make_values(x, others, begun, keys, query, bias):
    blocks, span, hd = keys.shape
    here = pl.BlockSpec(memory_space=pltpu.VMEM)
    return pl.pallas_call(
        values_kernel,
        out_shape=pltpu.HBM((blocks, span + EXTRA, hd), BF16),
        in_specs=[here] * 6 + [pl.BlockSpec(memory_space=pltpu.SMEM)],
        compiler_params=vmem(24),
        name="make_values",
    )(*on_chip(x), others[0], *on_chip(others[1], begun), keys, *on_chip(query), bias)


def store_kernel(rows_ref, out_ref, sem):
    copy = pltpu.make_async_copy(rows_ref, out_ref, sem)
    copy.start()
    copy.wait()


def store(rows):
    return pl.pallas_call(
        store_kernel,
        out_shape=pltpu.HBM(rows.shape, rows.dtype),
        in_specs=[pl.BlockSpec(memory_space=pl.ANY)],
        out_specs=pl.BlockSpec(memory_space=pl.ANY),
        scratch_shapes=[pltpu.SemaphoreType.DMA],
        compiler_params=vmem(4),
        name="store",
    )(rows)


def join_first_kernel(rows_ref, out_ref):
    count = rows_ref.shape[0]
    shape = (2, rows_ref.shape[2])
    read, log_later = jnp.zeros(shape, F32), jnp.zeros(shape, F32)
    for n in reversed(range(count)):
        rows = rows_ref[n, rows_ref.shape[1] - EXTRA :].astype(F32)
        read += jnp.exp(log_later) * (rows[0:2] + rows[2:4])
        log_later += rows[4:6] + rows[6:8]
    for n in range(out_ref.shape[0]):
        out_ref[n, 0:2] = read
        out_ref[n, 2:4] = log_later


def join_last_kernel(rows_ref, out_ref):
    count = rows_ref.shape[0]
    shape = (2, rows_ref.shape[2])
    read, log_later = jnp.zeros(shape, F32), jnp.zeros(shape, F32)
    for n in reversed(range(count)):
        read += jnp.exp(log_later) * rows_ref[n, 0:2]
        log_later += rows_ref[n, 2:4]
    out_ref[...] = read


def join_first(received, copies):
    return pl.pallas_call(
        join_first_kernel,
        out_shape=jax.ShapeDtypeStruct((copies, 4, received.shape[2]), F32),
        compiler_params=vmem(8),
        name="join_first",
    )(*on_chip(received))


def join_last(pieces):
    return pl.pallas_call(
        join_last_kernel,
        out_shape=jax.ShapeDtypeStruct((2, pieces.shape[2]), F32),
        compiler_params=vmem(4),
        name="join_last",
    )(*on_chip(pieces))


def shards(tokens, in_gain, w_key, w_value, k_gain, new_query, q_gain, stick_bias):
    seq_count, tok_seq, model_width = tokens.shape
    head_dim = k_gain.shape[0]
    heads = stick_bias.shape[0]
    kv_heads = w_key.shape[1] // head_dim
    per_group = heads // kv_heads
    seqs = seq_count // 2
    trade = functools.partial(lax.ppermute, axis_name="c", perm=[(0, 1), (1, 0)])
    ys, xs = lax.axis_size("y"), lax.axis_size("x")
    pieces = along_z(w_key, w_value)
    kept, sent = norm_halves(tokens, in_gain)
    early, late = spread(pieces, ys * xs)
    came = trade(sent)
    early = lax.all_to_all(early, SP, 0, 0, tiled=True)
    x, query = arrange(kept, came, new_query, q_gain, kv_heads)
    x = x.reshape(2, seq_count * tok_seq, model_width // 2)
    early = early.reshape(ys, xs, -1, head_dim)
    early_other = trade(early)
    begun = partial_product(x, (early,))
    keys, early_other = make_keys(x, early_other, begun, k_gain, seqs)
    got_keys = lax.all_to_all(keys, "z", 0, 0, tiled=True)
    late = lax.all_gather(late, SP).reshape(ys, xs, -1, head_dim)
    late_other = trade(late)
    begun = partial_product(x, (early, late))
    values = make_values(x, (early_other, late_other), begun, keys, query, stick_bias)
    got_values = lax.all_to_all(values, "z", 0, 0, tiled=True)
    stored = store(got_keys)
    joined = join_first(got_values, ys * xs)
    everything = lax.all_to_all(joined, SP, 0, 0, tiled=True)
    read = join_last(everything)
    span = 2 * tok_seq
    positions = got_keys.shape[0] * span
    key_cache = stored.reshape(1, positions, head_dim)
    value_cache = got_values[:, :span].reshape(1, positions, head_dim)
    return (key_cache, value_cache, read.reshape(1, per_group * head_dim))


def solution(mesh):
    grid = Mesh(mesh.devices.reshape(4, 4, 16, 2), ("y", "x", "z", "c"))
    tp = ("z", "c")
    return jax.shard_map(
        shards,
        mesh=grid,
        in_specs=(
            P(None, ("y", "x", "z", "c"), None),
            P(),
            P(tp, None),
            P(tp, None),
            P(),
            P(),
            P(),
            P(),
        ),
        out_specs=(P(tp, SP, None), P(tp, SP, None), P(tp, None)),
        check_vma=False,
    )
```

```python
import functools

import jax
import jax.numpy as jnp
from jax import lax
from jax.experimental import pallas as pl
from jax.experimental.pallas import tpu as pltpu
from jax.sharding import Mesh
from jax.sharding import PartitionSpec as P

NORM_EPS = 1e-06
SP = ("y", "x")
EXTRA = 8
F32 = jnp.float32
BF16 = jnp.bfloat16


def root_norm(values, scaling):
    inverse = lax.rsqrt(jnp.mean(values * values, axis=-1, keepdims=True) + NORM_EPS)
    return values * inverse * scaling


def to_all(piece, axis):
    count = lax.axis_size(axis)
    return lax.all_to_all(
        jnp.broadcast_to(piece[None], (count, *piece.shape)), axis, 0, 0, tiled=True
    )


def along_z(w_key, w_value):
    rows = w_key.shape[0] // lax.axis_size("x")
    width = w_key.shape[1] // lax.axis_size("y")
    at = (lax.axis_index("x") * rows, lax.axis_index("y") * width)
    parts = [lax.dynamic_slice(w, at, (rows, width)) for w in (w_key, w_value)]
    return to_all(jnp.stack(parts), "z")


def norm_kernel(tokens_ref, gain_ref, kept_ref, sent_ref):
    core = lax.axis_index("c")
    gain = gain_ref[...]
    kept_ref[0] = root_norm(tokens_ref[core].astype(F32), gain).astype(BF16)
    sent_ref[0] = root_norm(tokens_ref[1 - core].astype(F32), gain).astype(BF16)


def norm_halves(tokens, in_gain):
    seq_count, length, model = tokens.shape
    half = pltpu.HBM((seq_count // 2, length, model), BF16)
    block = pl.BlockSpec((1, length, model), lambda i: (i, 0, 0))
    return pl.pallas_call(
        norm_kernel,
        grid=(seq_count // 2,),
        out_shape=(half, half),
        in_specs=[
            pl.BlockSpec((2, length, model), lambda i: (i, 0, 0)),
            pl.BlockSpec((1, model), lambda i: (0, 0)),
        ],
        out_specs=(block, block),
        compiler_params=vmem(16),
        name="norm_halves",
    )(*off_chip(tokens, in_gain.reshape(1, model)))


def spread_kernel(pieces_ref, early_ref, late_ref):
    zs = pieces_ref.shape[0]
    early = early_ref.shape[1] - zs
    for n in range(early_ref.shape[0]):
        early_ref[n, :zs] = pieces_ref[:, 0]
        early_ref[n, zs:] = pieces_ref[:early, 1]
    late_ref[...] = pieces_ref[early:, 1]


def spread(pieces, count):
    zs, _, rows, width = pieces.shape
    early = zs // 16
    return pl.pallas_call(
        spread_kernel,
        out_shape=(
            jax.ShapeDtypeStruct((count, zs + early, rows, width), pieces.dtype),
            jax.ShapeDtypeStruct((zs - early, rows, width), pieces.dtype),
        ),
        compiler_params=vmem(8),
        name="spread",
    )(*on_chip(pieces))


def vmem(mib):
    return pltpu.CompilerParams(vmem_limit_bytes=mib * 1024 * 1024)


def on_chip(*arrays):
    return tuple(pltpu.with_memory_space_constraint(a, pltpu.VMEM) for a in arrays)


def off_chip(*arrays):
    return tuple(pltpu.with_memory_space_constraint(a, pltpu.HBM) for a in arrays)


def high_low(values):
    high = values.astype(BF16)
    return high, (values - high.astype(F32)).astype(BF16)


def arrange_kernel(
    kept_hbm, came_hbm, query_ref, gain_ref, x_ref, grouped_ref, kept_ref, came_ref, sems
):
    core = lax.axis_index("c")
    loads = [
        pltpu.make_async_copy(kept_hbm, kept_ref, sems.at[0]),
        pltpu.make_async_copy(came_hbm, came_ref, sems.at[1]),
    ]
    for load in loads:
        load.start()
    seqs, length, model = kept_ref.shape
    hd = gain_ref.shape[1]
    heads = query_ref.shape[1] // hd
    kv_heads = grouped_ref.shape[2] // hd
    zs, xs = lax.axis_size("z"), lax.axis_size("x")
    held = model // zs // 2
    rows = held // xs
    part = hd // rows
    deep = part * 2 * held
    source = lax.broadcasted_iota(jnp.int32, (deep, 2 * hd), 0)
    column = lax.broadcasted_iota(jnp.int32, (deep, 2 * hd), 1)
    inside = column % hd
    offset = source - (inside // rows) * (2 * held) - inside % rows - (column // hd) * rows

    query = query_ref[...].astype(F32)
    row = lax.broadcasted_iota(jnp.int32, (heads, hd), 0)
    per_group = heads // kv_heads
    for i in range(seqs):
        mine = jnp.where(core == 0, query[2 * i : 2 * i + 1], query[2 * i + 1 : 2 * i + 2])
        for g in range(kv_heads):
            block = jnp.zeros((heads, hd), F32)
            for j in range(g * per_group, (g + 1) * per_group):
                head = root_norm(mine[:, j * hd : (j + 1) * hd], gain_ref[...])
                block = jnp.where(row == j, head, block)
            grouped_ref[i, :, g * hd : (g + 1) * hd] = block.astype(BF16)
    for load in loads:
        load.wait()
    kept = kept_ref[...].reshape(seqs * length, model)
    came = came_ref[...].reshape(seqs * length, model)
    for half in range(2):
        for r in range(0, xs, 2):
            pick = (offset == half * held + r * rows).astype(BF16)
            for n in range(zs // part):
                for values, at in ((kept, core), (came, 1 - core)):
                    moved = jnp.dot(
                        values[:, n * deep : (n + 1) * deep], pick, preferred_element_type=F32
                    ).astype(BF16)
                    for k in range(2):
                        start = (r + k) * zs * rows + n * hd
                        x_ref[half, at, :, start : start + hd] = moved[:, k * hd : (k + 1) * hd]


def arrange(kept, came, new_query, q_gain, kv_heads):
    seqs, length, model = kept.shape
    hd = q_gain.shape[0]
    heads = new_query.shape[1] // hd
    return pl.pallas_call(
        arrange_kernel,
        out_shape=(
            pltpu.VMEM((2, 2, seqs * length, model // 2), BF16),
            pltpu.VMEM((seqs, heads, kv_heads * hd), BF16),
        ),
        in_specs=[pl.BlockSpec(memory_space=pl.ANY)] * 2
        + [pl.BlockSpec(memory_space=pltpu.VMEM)] * 2,
        scratch_shapes=[
            pltpu.VMEM(kept.shape, BF16),
            pltpu.VMEM(kept.shape, BF16),
            pltpu.SemaphoreType.DMA((2,)),
        ],
        compiler_params=vmem(32),
        name="arrange",
    )(*off_chip(kept), came, new_query, q_gain.reshape(1, hd))


def two_heads(refs, head):
    columns = []
    for g in (head, head + 1):
        blocks = [ref[g, n, first:last] for n in range(refs[0][0].shape[1]) for ref, first, last in refs]
        columns.append(jnp.concatenate(blocks, axis=0))
    return jnp.concatenate(columns, axis=1)


def key_part(early_ref, held):
    return ((early_ref, 0, held),)


def value_parts(early_ref, late_ref, held):
    first = held if early_ref.shape[2] > held else 0
    return ((early_ref, first, early_ref.shape[2]), (late_ref, 0, late_ref.shape[2]))


def partial_kernel(*refs):
    x_ref, *rows_refs, out_ref = refs
    x = x_ref[lax.axis_index("c")]
    heads, count, _, hd = rows_refs[0].shape
    held = x.shape[1] // count
    parts = key_part(*rows_refs, held) if len(rows_refs) == 1 else value_parts(*rows_refs, held)
    for g in range(0, heads, 2):
        out_ref[:, g * hd : (g + 2) * hd] = jnp.dot(
            x, two_heads(parts, g), preferred_element_type=F32
        )


def partial_product(x, rows):
    width = rows[0].shape[0] * rows[0].shape[-1]
    return pl.pallas_call(
        partial_kernel,
        out_shape=pltpu.VMEM((x.shape[1], width), F32),
        compiler_params=vmem(16),
        name="partial",
    )(*on_chip(x), *rows)


def place(ref, seqs, length, g, head):
    for n in range(2 * seqs):
        h, i = divmod(n, seqs)
        ref[g * seqs + i, h * length : (h + 1) * length, :] = head[n * length : (n + 1) * length]


def keys_kernel(x_ref, rows_ref, begun_ref, gain_ref, key_ref, rest_ref):
    x = x_ref[1 - lax.axis_index("c")]
    gain = gain_ref[...]
    kv_heads, hd = rows_ref.shape[0], gain.shape[1]
    held = x.shape[1] // rows_ref.shape[1]
    seqs = key_ref.shape[0] // kv_heads
    for g in range(0, kv_heads, 2):
        raw = begun_ref[:, g * hd : (g + 2) * hd] + jnp.dot(
            x, two_heads(key_part(rows_ref, held), g), preferred_element_type=F32
        )
        for k in range(2):
            head = root_norm(raw[:, k * hd : (k + 1) * hd], gain).astype(BF16)
            place(key_ref, seqs, key_ref.shape[1] // 2, g + k, head)
    rest_ref[...] = rows_ref[:, :, held:]


def make_keys(x, other, begun, gain, seqs):
    kv_heads, parts, rows, hd = other.shape
    rest = rows - x.shape[2] // parts
    return pl.pallas_call(
        keys_kernel,
        out_shape=(
            pltpu.HBM((kv_heads * seqs, x.shape[1] // seqs, hd), BF16),
            pltpu.HBM((kv_heads, parts, rest, hd), BF16),
        ),
        compiler_params=vmem(16),
        name="make_keys",
    )(*on_chip(x, other, begun), gain.reshape(1, hd))


def values_kernel(x_ref, early_ref, late_ref, begun_ref, key_ref, query_ref, bias_ref, value_ref):
    core = lax.axis_index("c")
    seqs, heads, width = query_ref.shape
    hd = key_ref.shape[2]
    span = key_ref.shape[1]
    kv_heads = width // hd
    per_group = heads // kv_heads
    x = x_ref[1 - core]
    held = x.shape[1] // early_ref.shape[1]

    row = lax.broadcasted_iota(jnp.int32, (heads, 1), 0)
    bias = jnp.zeros((heads, 1), F32)
    for j in range(heads):
        bias = jnp.where(row == j, bias_ref[j], bias)
    scores = []
    for i in range(seqs):
        total = jnp.zeros((heads, span), F32)
        for g in range(kv_heads):
            total += lax.dot_general(
                query_ref[i, :, g * hd : (g + 1) * hd],
                key_ref[g * seqs + i],
                (((1,), (1,)), ((), ())),
                preferred_element_type=F32,
            )
        scores.append(total * (hd**-0.5) + bias)
    scores = jnp.concatenate(scores, axis=0)
    log_keep = -(jnp.maximum(scores, 0.0) + jnp.log1p(jnp.exp(-jnp.abs(scores))))
    first = lax.broadcasted_iota(jnp.int32, (span, span), 0)
    second = lax.broadcasted_iota(jnp.int32, (span, span), 1)
    later = (first > second).astype(BF16)
    after = jnp.zeros(scores.shape, F32)
    rest = log_keep
    for _ in range(3):
        part = rest.astype(BF16)
        rest = rest - part.astype(F32)
        after += jnp.dot(part, later, preferred_element_type=F32)
    weight_high, weight_low = high_low(jnp.exp(scores + log_keep + after))
    total_high, total_low = high_low(jnp.sum(log_keep, axis=1, keepdims=True))

    for g in range(0, kv_heads, 2):
        raw = begun_ref[:, g * hd : (g + 2) * hd] + jnp.dot(
            x, two_heads(value_parts(early_ref, late_ref, held), g), preferred_element_type=F32
        )
        for k in range(2):
            place(value_ref, seqs, span // 2, g + k, raw[:, k * hd : (k + 1) * hd].astype(BF16))

    put = lax.broadcasted_iota(jnp.int32, (EXTRA, 4 * heads), 0)
    take = lax.broadcasted_iota(jnp.int32, (EXTRA, 4 * heads), 1)
    for i in range(seqs):
        at = slice(i * heads, (i + 1) * heads)
        for g in range(kv_heads):
            values = value_ref[g * seqs + i, 0:span]
            read = jnp.dot(weight_high[at], values, preferred_element_type=F32) + jnp.dot(
                weight_low[at], values, preferred_element_type=F32
            )
            read_high, read_low = high_low(read)
            stacked = jnp.concatenate(
                [
                    read_high.astype(F32),
                    read_low.astype(F32),
                    jnp.broadcast_to(total_high[at].astype(F32), read.shape),
                    jnp.broadcast_to(total_low[at].astype(F32), read.shape),
                ],
                axis=0,
            ).astype(BF16)
            pick = (
                take == (put // per_group) * heads + g * per_group + put % per_group
            ).astype(BF16)
            value_ref[g * seqs + i, span:, :] = jnp.dot(
                pick, stacked, preferred_element_type=F32
            ).astype(BF16)


def make_values(x, others, begun, keys, query, bias):
    blocks, span, hd = keys.shape
    here = pl.BlockSpec(memory_space=pltpu.VMEM)
    return pl.pallas_call(
        values_kernel,
        out_shape=pltpu.HBM((blocks, span + EXTRA, hd), BF16),
        in_specs=[here] * 6 + [pl.BlockSpec(memory_space=pltpu.SMEM)],
        compiler_params=vmem(24),
        name="make_values",
    )(*on_chip(x), others[0], *on_chip(others[1], begun), keys, *on_chip(query), bias)


def store_kernel(rows_ref, out_ref):
    out_ref[...] = rows_ref[...]


def store(rows):
    blocks, span, hd = rows.shape
    spec = pl.BlockSpec((blocks // 4, span, hd), lambda n: (n, 0, 0))
    return pl.pallas_call(
        store_kernel,
        grid=(4,),
        out_shape=pltpu.HBM(rows.shape, rows.dtype),
        in_specs=[spec],
        out_specs=spec,
        compiler_params=vmem(8),
        name="store",
    )(*off_chip(rows))


def join_first_kernel(rows_ref, out_ref):
    count = rows_ref.shape[0]
    shape = (2, rows_ref.shape[2])
    read, log_later = jnp.zeros(shape, F32), jnp.zeros(shape, F32)
    for n in reversed(range(count)):
        rows = rows_ref[n, rows_ref.shape[1] - EXTRA :].astype(F32)
        read += jnp.exp(log_later) * (rows[0:2] + rows[2:4])
        log_later += rows[4:6] + rows[6:8]
    for n in range(out_ref.shape[0]):
        out_ref[n, 0:2] = read
        out_ref[n, 2:4] = log_later


def join_last_kernel(rows_ref, out_ref):
    count = rows_ref.shape[0]
    shape = (2, rows_ref.shape[2])
    read, log_later = jnp.zeros(shape, F32), jnp.zeros(shape, F32)
    for n in reversed(range(count)):
        read += jnp.exp(log_later) * rows_ref[n, 0:2]
        log_later += rows_ref[n, 2:4]
    out_ref[...] = read


def join_first(received, copies):
    return pl.pallas_call(
        join_first_kernel,
        out_shape=jax.ShapeDtypeStruct((copies, 4, received.shape[2]), F32),
        compiler_params=vmem(8),
        name="join_first",
    )(*on_chip(received))


def join_last(pieces):
    return pl.pallas_call(
        join_last_kernel,
        out_shape=jax.ShapeDtypeStruct((2, pieces.shape[2]), F32),
        compiler_params=vmem(4),
        name="join_last",
    )(*on_chip(pieces))


def shards(tokens, in_gain, w_key, w_value, k_gain, new_query, q_gain, stick_bias):
    seq_count, tok_seq, model_width = tokens.shape
    head_dim = k_gain.shape[0]
    heads = stick_bias.shape[0]
    kv_heads = w_key.shape[1] // head_dim
    per_group = heads // kv_heads
    seqs = seq_count // 2
    trade = functools.partial(lax.ppermute, axis_name="c", perm=[(0, 1), (1, 0)])
    ys, xs = lax.axis_size("y"), lax.axis_size("x")
    pieces = along_z(w_key, w_value)
    kept, sent = norm_halves(tokens, in_gain)
    early, late = spread(pieces, ys * xs)
    came = trade(sent)
    early = lax.all_to_all(early, SP, 0, 0, tiled=True)
    x, query = arrange(kept, came, new_query, q_gain, kv_heads)
    x = x.reshape(2, seq_count * tok_seq, model_width // 2)
    early = early.reshape(ys, xs, -1, head_dim)
    early_other = trade(early)
    begun = partial_product(x, (early,))
    keys, early_other = make_keys(x, early_other, begun, k_gain, seqs)
    got_keys = lax.all_to_all(keys, "z", 0, 0, tiled=True)
    late = lax.all_gather(late, SP).reshape(ys, xs, -1, head_dim)
    late_other = trade(late)
    begun = partial_product(x, (early, late))
    values = make_values(x, (early_other, late_other), begun, keys, query, stick_bias)
    got_values = lax.all_to_all(values, "z", 0, 0, tiled=True)
    stored = store(got_keys)
    joined = join_first(got_values, ys * xs)
    everything = lax.all_to_all(joined, SP, 0, 0, tiled=True)
    read = join_last(everything)
    span = 2 * tok_seq
    positions = got_keys.shape[0] * span
    key_cache = stored.reshape(1, positions, head_dim)
    value_cache = got_values[:, :span].reshape(1, positions, head_dim)
    return (key_cache, value_cache, read.reshape(1, per_group * head_dim))


def solution(mesh):
    grid = Mesh(mesh.devices.reshape(4, 4, 16, 2), ("y", "x", "z", "c"))
    tp = ("z", "c")
    return jax.shard_map(
        shards,
        mesh=grid,
        in_specs=(
            P(None, ("y", "x", "z", "c"), None),
            P(),
            P(tp, None),
            P(tp, None),
            P(),
            P(),
            P(),
            P(),
        ),
        out_specs=(P(tp, SP, None), P(tp, SP, None), P(tp, None)),
        check_vma=False,
    )
```

```python
import functools

import jax
import jax.numpy as jnp
from jax import lax
from jax.experimental import pallas as pl
from jax.experimental.pallas import tpu as pltpu
from jax.sharding import Mesh
from jax.sharding import PartitionSpec as P

NORM_EPS = 1e-06
SP = ("y", "x")
EXTRA = 8
F32 = jnp.float32
BF16 = jnp.bfloat16


def root_norm(values, scaling):
    inverse = lax.rsqrt(jnp.mean(values * values, axis=-1, keepdims=True) + NORM_EPS)
    return values * inverse * scaling


def to_all(piece, axis):
    count = lax.axis_size(axis)
    return lax.all_to_all(
        jnp.broadcast_to(piece[None], (count, *piece.shape)), axis, 0, 0, tiled=True
    )


def along_z(w_key, w_value):
    rows = w_key.shape[0] // lax.axis_size("x")
    width = w_key.shape[1] // lax.axis_size("y")
    at = (lax.axis_index("x") * rows, lax.axis_index("y") * width)
    parts = [lax.dynamic_slice(w, at, (rows, width)) for w in (w_key, w_value)]
    return to_all(jnp.stack(parts), "z")


def norm_kernel(tokens_ref, gain_ref, w_key_ref, w_value_ref, kept_ref, sent_ref):
    core = lax.axis_index("c")
    step = pl.program_id(0)
    gain = gain_ref[...]
    length = kept_ref.shape[1]
    extra = sent_ref.shape[1] - length
    kept_ref[0] = root_norm(tokens_ref[core].astype(F32), gain).astype(BF16)
    sent_ref[0, :length] = root_norm(tokens_ref[1 - core].astype(F32), gain).astype(BF16)
    width = w_key_ref.shape[1]
    across = sent_ref.shape[2] // width
    half = pl.num_programs(0) // 2
    at = pl.multiple_of(lax.rem(step, half) * (extra * across), 32)
    rows = jnp.where(
        step < half,
        w_key_ref[pl.ds(at, extra * across), :],
        w_value_ref[pl.ds(at, extra * across), :],
    )
    for m in range(across):
        sent_ref[0, length:, m * width : (m + 1) * width] = rows[m * extra : (m + 1) * extra]


def norm_halves(tokens, in_gain, w_key, w_value):
    seq_count, length, model = tokens.shape
    seqs = seq_count // 2
    extra = 2 * w_key.size // (seqs * model)
    whole = pl.BlockSpec(w_key.shape, lambda i: (0, 0))
    return pl.pallas_call(
        norm_kernel,
        grid=(seqs,),
        out_shape=(
            pltpu.HBM((seqs, length, model), BF16),
            pltpu.HBM((seqs, length + extra, model), BF16),
        ),
        in_specs=[
            pl.BlockSpec((2, length, model), lambda i: (i, 0, 0)),
            pl.BlockSpec((1, model), lambda i: (0, 0)),
            whole,
            whole,
        ],
        out_specs=(
            pl.BlockSpec((1, length, model), lambda i: (i, 0, 0)),
            pl.BlockSpec((1, length + extra, model), lambda i: (i, 0, 0)),
        ),
        compiler_params=vmem(16),
        name="norm_halves",
    )(*off_chip(tokens, in_gain.reshape(1, model), w_key, w_value))


def from_here(distance):
    return lax.rem(lax.axis_index("z") + distance, lax.axis_size("z"))


def spread_kernel(pieces_ref, early_ref, late_ref):
    for k in range(late_ref.shape[0]):
        at = from_here(k + 1)
        piece = pieces_ref[at, 0]
        for n in range(early_ref.shape[0]):
            early_ref[n, k] = piece
        late_ref[k] = pieces_ref[at, 1]


def spread(pieces, count):
    zs, _, rows, width = pieces.shape
    return pl.pallas_call(
        spread_kernel,
        out_shape=(
            jax.ShapeDtypeStruct((count, zs - 1, rows, width), pieces.dtype),
            jax.ShapeDtypeStruct((zs - 1, rows, width), pieces.dtype),
        ),
        compiler_params=vmem(8),
        name="spread",
    )(*on_chip(pieces))


def vmem(mib):
    return pltpu.CompilerParams(vmem_limit_bytes=mib * 1024 * 1024)


def on_chip(*arrays):
    return tuple(pltpu.with_memory_space_constraint(a, pltpu.VMEM) for a in arrays)


def off_chip(*arrays):
    return tuple(pltpu.with_memory_space_constraint(a, pltpu.HBM) for a in arrays)


def high_low(values):
    high = values.astype(BF16)
    return high, (values - high.astype(F32)).astype(BF16)


def arranged(tokens_ref, x_ref):
    half, _, model_half = x_ref.shape
    model = half * model_half
    zs, xs = lax.axis_size("z"), lax.axis_size("x")
    held = model // zs // 2
    rows = held // xs
    hd = 128
    part = hd // rows
    deep = part * 2 * held
    source = lax.broadcasted_iota(jnp.int32, (deep, 2 * hd), 0)
    column = lax.broadcasted_iota(jnp.int32, (deep, 2 * hd), 1)
    inside = column % hd
    offset = source - (inside // rows) * (2 * held) - inside % rows - (column // hd) * rows
    seqs = tokens_ref.shape[0]
    length = x_ref.shape[1] // seqs
    groups = []
    for n in range(zs // part):
        columns = [
            tokens_ref[:, :length, pl.ds(pl.multiple_of(from_here(n * part + k) * hd, hd), hd)]
            for k in range(part)
        ]
        groups.append(
            jnp.concatenate([c.reshape(seqs * length, hd) for c in columns], axis=1)
        )
    for h in range(half):
        for r in range(0, xs, 2):
            pick = (offset == h * held + r * rows).astype(BF16)
            for n in range(zs // part):
                moved = jnp.dot(groups[n], pick, preferred_element_type=F32).astype(BF16)
                for k in range(2):
                    start = (r + k) * zs * rows + n * hd
                    x_ref[h, :, start : start + hd] = moved[:, k * hd : (k + 1) * hd]


def group_queries(query_ref, gain_ref, grouped_ref):
    core = lax.axis_index("c")
    hd = gain_ref.shape[1]
    seqs, heads, width = grouped_ref.shape
    kv_heads = width // hd
    query = query_ref[...].astype(F32)
    row = lax.broadcasted_iota(jnp.int32, (heads, hd), 0)
    per_group = heads // kv_heads
    for i in range(seqs):
        mine = jnp.where(core == 0, query[2 * i : 2 * i + 1], query[2 * i + 1 : 2 * i + 2])
        for g in range(kv_heads):
            block = jnp.zeros((heads, hd), F32)
            for j in range(g * per_group, (g + 1) * per_group):
                head = root_norm(mine[:, j * hd : (j + 1) * hd], gain_ref[...])
                block = jnp.where(row == j, head, block)
            grouped_ref[i, :, g * hd : (g + 1) * hd] = block.astype(BF16)


def arrange_kept_kernel(kept_hbm, query_ref, gain_ref, x_ref, grouped_ref, kept_ref, sem):
    load = pltpu.make_async_copy(kept_hbm, kept_ref, sem)
    load.start()
    group_queries(query_ref, gain_ref, grouped_ref)
    load.wait()
    arranged(kept_ref, x_ref)


def arrange_came_kernel(came_ref, x_ref, shards_ref):
    arranged(came_ref, x_ref)
    seqs, rows, model = came_ref.shape
    length = x_ref.shape[1] // seqs
    extra = rows - length
    _, held, width = shards_ref.shape
    for i in range(seqs):
        for m in range(model // width):
            which, at = divmod((i * (model // width) + m) * extra, held)
            shards_ref[which, at : at + extra] = came_ref[
                i, length:, m * width : (m + 1) * width
            ]


def arrange_kept(kept, new_query, q_gain, kv_heads):
    seqs, length, model = kept.shape
    hd = q_gain.shape[0]
    heads = new_query.shape[1] // hd
    return pl.pallas_call(
        arrange_kept_kernel,
        out_shape=(
            pltpu.VMEM((2, seqs * length, model // 2), BF16),
            pltpu.VMEM((seqs, heads, kv_heads * hd), BF16),
        ),
        in_specs=[pl.BlockSpec(memory_space=pl.ANY)]
        + [pl.BlockSpec(memory_space=pltpu.VMEM)] * 2,
        scratch_shapes=[pltpu.VMEM(kept.shape, BF16), pltpu.SemaphoreType.DMA],
        compiler_params=vmem(20),
        name="arrange_kept",
    )(*off_chip(kept), new_query, q_gain.reshape(1, hd))


def arrange_came(came, length, shard):
    seqs, _, model = came.shape
    return pl.pallas_call(
        arrange_came_kernel,
        out_shape=(
            pltpu.VMEM((2, seqs * length, model // 2), BF16),
            pltpu.VMEM((2, *shard), BF16),
        ),
        compiler_params=vmem(20),
        name="arrange_came",
    )(came)


def both(refs, core):
    return jnp.concatenate([ref[core] for ref in refs], axis=0)


def two_heads(shard, rows_ref, head):
    parts, hd = rows_ref.shape[1], rows_ref.shape[3]
    rows = shard.shape[0] // parts
    columns = []
    for g in (head, head + 1):
        blocks = []
        for n in range(parts):
            blocks.append(shard[n * rows : (n + 1) * rows, g * hd : (g + 1) * hd])
            blocks.append(rows_ref[g, n])
        columns.append(jnp.concatenate(blocks, axis=0))
    return jnp.concatenate(columns, axis=1)


def partial_kernel(kept_ref, came_ref, shard_ref, rows_ref, out_ref):
    x = both((kept_ref, came_ref), lax.axis_index("c"))
    heads, _, _, hd = rows_ref.shape
    shard = shard_ref[...]
    for g in range(0, heads, 2):
        out_ref[:, g * hd : (g + 2) * hd] = jnp.dot(
            x, two_heads(shard, rows_ref, g), preferred_element_type=F32
        )


def partial_product(x, shard, rows):
    return pl.pallas_call(
        partial_kernel,
        out_shape=pltpu.VMEM((2 * x[0].shape[1], shard.shape[1]), F32),
        compiler_params=vmem(16),
        name="partial",
    )(*on_chip(*x), shard, rows)


def place(ref, seqs, length, g, head):
    core = lax.axis_index("c")
    for n in range(2 * seqs):
        half, i = divmod(n, seqs)
        at = pl.multiple_of((core if half == 0 else 1 - core) * length, 32)
        ref[g * seqs + i, pl.ds(at, length), :] = head[n * length : (n + 1) * length]


def keys_kernel(kept_ref, came_ref, shards_ref, rows_ref, begun_ref, gain_ref, key_ref):
    x = both((kept_ref, came_ref), 1 - lax.axis_index("c"))
    gain = gain_ref[...]
    shard = shards_ref[0]
    kv_heads, hd = rows_ref.shape[0], gain.shape[1]
    seqs = key_ref.shape[0] // kv_heads
    for g in range(0, kv_heads, 2):
        raw = begun_ref[:, g * hd : (g + 2) * hd] + jnp.dot(
            x, two_heads(shard, rows_ref, g), preferred_element_type=F32
        )
        for k in range(2):
            head = root_norm(raw[:, k * hd : (k + 1) * hd], gain).astype(BF16)
            place(key_ref, seqs, key_ref.shape[1] // 2, g + k, head)


def make_keys(x, shards_other, other, begun, gain, seqs):
    kv_heads, hd = other.shape[0], other.shape[3]
    return pl.pallas_call(
        keys_kernel,
        out_shape=pltpu.HBM((kv_heads * seqs, 2 * x[0].shape[1] // seqs, hd), BF16),
        compiler_params=vmem(16),
        name="make_keys",
    )(*on_chip(*x), shards_other, *on_chip(other, begun), gain.reshape(1, hd))


def values_kernel(
    kept_ref, came_ref, shards_ref, rows_ref, begun_ref, key_ref, query_ref, bias_ref, value_ref
):
    core = lax.axis_index("c")
    seqs, heads, width = query_ref.shape
    hd = key_ref.shape[2]
    span = key_ref.shape[1]
    kv_heads = width // hd
    per_group = heads // kv_heads
    x = both((kept_ref, came_ref), 1 - core)
    shard = shards_ref[1]

    row = lax.broadcasted_iota(jnp.int32, (heads, 1), 0)
    bias = jnp.zeros((heads, 1), F32)
    for j in range(heads):
        bias = jnp.where(row == j, bias_ref[j], bias)
    scores = []
    for i in range(seqs):
        total = jnp.zeros((heads, span), F32)
        for g in range(kv_heads):
            total += lax.dot_general(
                query_ref[i, :, g * hd : (g + 1) * hd],
                key_ref[g * seqs + i],
                (((1,), (1,)), ((), ())),
                preferred_element_type=F32,
            )
        scores.append(total * (hd**-0.5) + bias)
    scores = jnp.concatenate(scores, axis=0)
    log_keep = -(jnp.maximum(scores, 0.0) + jnp.log1p(jnp.exp(-jnp.abs(scores))))
    first = lax.broadcasted_iota(jnp.int32, (span, span), 0)
    second = lax.broadcasted_iota(jnp.int32, (span, span), 1)
    later = (first > second).astype(BF16)
    after = jnp.zeros(scores.shape, F32)
    rest = log_keep
    for _ in range(3):
        part = rest.astype(BF16)
        rest = rest - part.astype(F32)
        after += jnp.dot(part, later, preferred_element_type=F32)
    weight_high, weight_low = high_low(jnp.exp(scores + log_keep + after))
    total_high, total_low = high_low(jnp.sum(log_keep, axis=1, keepdims=True))

    for g in range(0, kv_heads, 2):
        raw = begun_ref[:, g * hd : (g + 2) * hd] + jnp.dot(
            x, two_heads(shard, rows_ref, g), preferred_element_type=F32
        )
        for k in range(2):
            place(value_ref, seqs, span // 2, g + k, raw[:, k * hd : (k + 1) * hd].astype(BF16))

    put = lax.broadcasted_iota(jnp.int32, (EXTRA, 4 * heads), 0)
    take = lax.broadcasted_iota(jnp.int32, (EXTRA, 4 * heads), 1)
    for i in range(seqs):
        at = slice(i * heads, (i + 1) * heads)
        for g in range(kv_heads):
            values = value_ref[g * seqs + i, 0:span]
            read = jnp.dot(weight_high[at], values, preferred_element_type=F32) + jnp.dot(
                weight_low[at], values, preferred_element_type=F32
            )
            read_high, read_low = high_low(read)
            stacked = jnp.concatenate(
                [
                    read_high.astype(F32),
                    read_low.astype(F32),
                    jnp.broadcast_to(total_high[at].astype(F32), read.shape),
                    jnp.broadcast_to(total_low[at].astype(F32), read.shape),
                ],
                axis=0,
            ).astype(BF16)
            pick = (
                take == (put // per_group) * heads + g * per_group + put % per_group
            ).astype(BF16)
            value_ref[g * seqs + i, span:, :] = jnp.dot(
                pick, stacked, preferred_element_type=F32
            ).astype(BF16)


def make_values(x, shards_other, other, begun, keys, query, bias):
    blocks, span, hd = keys.shape
    here = pl.BlockSpec(memory_space=pltpu.VMEM)
    return pl.pallas_call(
        values_kernel,
        out_shape=pltpu.HBM((blocks, span + EXTRA, hd), BF16),
        in_specs=[here] * 7 + [pl.BlockSpec(memory_space=pltpu.SMEM)],
        compiler_params=vmem(24),
        name="make_values",
    )(*on_chip(*x), shards_other, *on_chip(other, begun), keys, *on_chip(query), bias)


def store_kernel(rows_ref, out_ref):
    out_ref[...] = rows_ref[...]


def store(rows):
    blocks, span, hd = rows.shape
    spec = pl.BlockSpec((blocks // 4, span, hd), lambda n: (n, 0, 0))
    return pl.pallas_call(
        store_kernel,
        grid=(4,),
        out_shape=pltpu.HBM(rows.shape, rows.dtype),
        in_specs=[spec],
        out_specs=spec,
        compiler_params=vmem(8),
        name="store",
    )(*off_chip(rows))


def join_first_kernel(rows_ref, out_ref):
    count = rows_ref.shape[0]
    shape = (2, rows_ref.shape[2])
    read, log_later = jnp.zeros(shape, F32), jnp.zeros(shape, F32)
    for n in reversed(range(count)):
        rows = rows_ref[n, rows_ref.shape[1] - EXTRA :].astype(F32)
        read += jnp.exp(log_later) * (rows[0:2] + rows[2:4])
        log_later += rows[4:6] + rows[6:8]
    for n in range(out_ref.shape[0]):
        out_ref[n, 0:2] = read
        out_ref[n, 2:4] = log_later


def join_last_kernel(rows_ref, out_ref):
    count = rows_ref.shape[0]
    shape = (2, rows_ref.shape[2])
    read, log_later = jnp.zeros(shape, F32), jnp.zeros(shape, F32)
    for n in reversed(range(count)):
        read += jnp.exp(log_later) * rows_ref[n, 0:2]
        log_later += rows_ref[n, 2:4]
    out_ref[...] = read


def join_first(received, copies):
    return pl.pallas_call(
        join_first_kernel,
        out_shape=jax.ShapeDtypeStruct((copies, 4, received.shape[2]), F32),
        compiler_params=vmem(8),
        name="join_first",
    )(*on_chip(received))


def join_last(pieces):
    return pl.pallas_call(
        join_last_kernel,
        out_shape=jax.ShapeDtypeStruct((2, pieces.shape[2]), F32),
        compiler_params=vmem(4),
        name="join_last",
    )(*on_chip(pieces))


def shards(tokens, in_gain, w_key, w_value, k_gain, new_query, q_gain, stick_bias):
    seq_count, tok_seq, _ = tokens.shape
    head_dim = k_gain.shape[0]
    heads = stick_bias.shape[0]
    kv_heads = w_key.shape[1] // head_dim
    per_group = heads // kv_heads
    seqs = seq_count // 2
    trade = functools.partial(lax.ppermute, axis_name="c", perm=[(0, 1), (1, 0)])
    ys, xs = lax.axis_size("y"), lax.axis_size("x")
    pieces = along_z(w_key, w_value)
    kept, sent = norm_halves(tokens, in_gain, w_key, w_value)
    early, late = spread(pieces, ys * xs)
    came = trade(sent)
    early = lax.all_to_all(early, SP, 0, 0, tiled=True)
    x_kept, query = arrange_kept(kept, new_query, q_gain, kv_heads)
    x_came, shards_other = arrange_came(came, tok_seq, w_key.shape)
    x = (x_kept, x_came)
    early = early.reshape(ys, xs, -1, head_dim)
    early_other = trade(early)
    begun = partial_product(x, w_key, early)
    keys = make_keys(x, shards_other, early_other, begun, k_gain, seqs)
    got_keys = lax.all_to_all(keys, "z", 0, 0, tiled=True)
    late = lax.all_gather(late, SP).reshape(ys, xs, -1, head_dim)
    late_other = trade(late)
    begun = partial_product(x, w_value, late)
    values = make_values(x, shards_other, late_other, begun, keys, query, stick_bias)
    got_values = lax.all_to_all(values, "z", 0, 0, tiled=True)
    stored = store(got_keys)
    joined = join_first(got_values, ys * xs)
    everything = lax.all_to_all(joined, SP, 0, 0, tiled=True)
    read = join_last(everything)
    span = 2 * tok_seq
    positions = got_keys.shape[0] * span
    key_cache = stored.reshape(1, positions, head_dim)
    value_cache = got_values[:, :span].reshape(1, positions, head_dim)
    return (key_cache, value_cache, read.reshape(1, per_group * head_dim))


def solution(mesh):
    grid = Mesh(mesh.devices.reshape(4, 4, 16, 2), ("y", "x", "z", "c"))
    tp = ("z", "c")
    return jax.shard_map(
        shards,
        mesh=grid,
        in_specs=(
            P(None, ("y", "x", "z", "c"), None),
            P(),
            P(tp, None),
            P(tp, None),
            P(),
            P(),
            P(),
            P(),
        ),
        out_specs=(P(tp, SP, None), P(tp, SP, None), P(tp, None)),
        check_vma=False,
    )
```

```python
import functools

import jax
import jax.numpy as jnp
from jax import lax
from jax.experimental import pallas as pl
from jax.experimental.pallas import tpu as pltpu
from jax.sharding import Mesh
from jax.sharding import PartitionSpec as P

NORM_EPS = 1e-06
SP = ("y", "x")
EXTRA = 8
F32 = jnp.float32
BF16 = jnp.bfloat16


def root_norm(values, scaling):
    inverse = lax.rsqrt(jnp.mean(values * values, axis=-1, keepdims=True) + NORM_EPS)
    return values * inverse * scaling


def to_all(piece, axis):
    count = lax.axis_size(axis)
    return lax.all_to_all(
        jnp.broadcast_to(piece[None], (count, *piece.shape)), axis, 0, 0, tiled=True
    )


def along_z(w_key, w_value):
    rows = w_key.shape[0] // lax.axis_size("x")
    width = w_key.shape[1] // lax.axis_size("y")
    at = (lax.axis_index("x") * rows, lax.axis_index("y") * width)
    parts = [lax.dynamic_slice(w, at, (rows, width)) for w in (w_key, w_value)]
    return to_all(jnp.stack(parts), "z")


def norm_kernel(tokens_ref, gain_ref, w_key_ref, w_value_ref, kept_ref, sent_ref):
    core = lax.axis_index("c")
    step = pl.program_id(0)
    gain = gain_ref[...]
    length = kept_ref.shape[1]
    extra = sent_ref.shape[1] - length
    kept_ref[0] = root_norm(tokens_ref[core].astype(F32), gain).astype(BF16)
    sent_ref[0, :length] = root_norm(tokens_ref[1 - core].astype(F32), gain).astype(BF16)
    width = w_key_ref.shape[1]
    across = sent_ref.shape[2] // width
    half = pl.num_programs(0) // 2
    at = pl.multiple_of(lax.rem(step, half) * (extra * across), 32)
    rows = jnp.where(
        step < half,
        w_key_ref[pl.ds(at, extra * across), :],
        w_value_ref[pl.ds(at, extra * across), :],
    )
    for m in range(across):
        sent_ref[0, length:, m * width : (m + 1) * width] = rows[m * extra : (m + 1) * extra]


def norm_halves(tokens, in_gain, w_key, w_value):
    seq_count, length, model = tokens.shape
    seqs = seq_count // 2
    extra = 2 * w_key.size // (seqs * model)
    whole = pl.BlockSpec(w_key.shape, lambda i: (0, 0))
    return pl.pallas_call(
        norm_kernel,
        grid=(seqs,),
        out_shape=(
            pltpu.HBM((seqs, length, model), BF16),
            pltpu.HBM((seqs, length + extra, model), BF16),
        ),
        in_specs=[
            pl.BlockSpec((2, length, model), lambda i: (i, 0, 0)),
            pl.BlockSpec((1, model), lambda i: (0, 0)),
            whole,
            whole,
        ],
        out_specs=(
            pl.BlockSpec((1, length, model), lambda i: (i, 0, 0)),
            pl.BlockSpec((1, length + extra, model), lambda i: (i, 0, 0)),
        ),
        compiler_params=vmem(16),
        name="norm_halves",
    )(*off_chip(tokens, in_gain.reshape(1, model), w_key, w_value))


def from_here(distance):
    return lax.rem(lax.axis_index("z") + distance, lax.axis_size("z"))


def spread_kernel(pieces_ref, early_ref, late_ref):
    for k in range(late_ref.shape[0]):
        at = from_here(k + 1)
        piece = pieces_ref[at, 0]
        for n in range(early_ref.shape[0]):
            early_ref[n, k] = piece
        late_ref[k] = pieces_ref[at, 1]


def spread(pieces, count):
    zs, _, rows, width = pieces.shape
    return pl.pallas_call(
        spread_kernel,
        out_shape=(
            jax.ShapeDtypeStruct((count, zs - 1, rows, width), pieces.dtype),
            jax.ShapeDtypeStruct((zs - 1, rows, width), pieces.dtype),
        ),
        compiler_params=vmem(8),
        name="spread",
    )(*on_chip(pieces))


def vmem(mib):
    return pltpu.CompilerParams(vmem_limit_bytes=mib * 1024 * 1024)


def on_chip(*arrays):
    return tuple(pltpu.with_memory_space_constraint(a, pltpu.VMEM) for a in arrays)


def off_chip(*arrays):
    return tuple(pltpu.with_memory_space_constraint(a, pltpu.HBM) for a in arrays)


def high_low(values):
    high = values.astype(BF16)
    return high, (values - high.astype(F32)).astype(BF16)


def arranged(tokens_ref, x_ref):
    half, _, model_half = x_ref.shape
    model = half * model_half
    zs, xs = lax.axis_size("z"), lax.axis_size("x")
    held = model // zs // 2
    rows = held // xs
    hd = 128
    part = hd // rows
    deep = part * 2 * held
    source = lax.broadcasted_iota(jnp.int32, (deep, 2 * hd), 0)
    column = lax.broadcasted_iota(jnp.int32, (deep, 2 * hd), 1)
    inside = column % hd
    offset = source - (inside // rows) * (2 * held) - inside % rows - (column // hd) * rows
    seqs = tokens_ref.shape[0]
    length = x_ref.shape[1] // seqs
    groups = []
    for n in range(zs // part):
        columns = [
            tokens_ref[:, :length, pl.ds(pl.multiple_of(from_here(n * part + k) * hd, hd), hd)]
            for k in range(part)
        ]
        groups.append(
            jnp.concatenate([c.reshape(seqs * length, hd) for c in columns], axis=1)
        )
    for h in range(half):
        for r in range(0, xs, 2):
            pick = (offset == h * held + r * rows).astype(BF16)
            for n in range(zs // part):
                moved = jnp.dot(groups[n], pick, preferred_element_type=F32).astype(BF16)
                for k in range(2):
                    start = (r + k) * zs * rows + n * hd
                    x_ref[h, :, start : start + hd] = moved[:, k * hd : (k + 1) * hd]


def group_queries(query_ref, gain_ref, grouped_ref):
    core = lax.axis_index("c")
    hd = gain_ref.shape[1]
    seqs, heads, width = grouped_ref.shape
    kv_heads = width // hd
    query = query_ref[...].astype(F32)
    row = lax.broadcasted_iota(jnp.int32, (heads, hd), 0)
    per_group = heads // kv_heads
    for i in range(seqs):
        mine = jnp.where(core == 0, query[2 * i : 2 * i + 1], query[2 * i + 1 : 2 * i + 2])
        for g in range(kv_heads):
            block = jnp.zeros((heads, hd), F32)
            for j in range(g * per_group, (g + 1) * per_group):
                head = root_norm(mine[:, j * hd : (j + 1) * hd], gain_ref[...])
                block = jnp.where(row == j, head, block)
            grouped_ref[i, :, g * hd : (g + 1) * hd] = block.astype(BF16)


def arrange_kept_kernel(kept_hbm, query_ref, gain_ref, x_ref, grouped_ref, kept_ref, sem):
    load = pltpu.make_async_copy(kept_hbm, kept_ref, sem)
    load.start()
    group_queries(query_ref, gain_ref, grouped_ref)
    load.wait()
    arranged(kept_ref, x_ref)


def arrange_came_kernel(came_ref, x_ref, shards_ref):
    arranged(came_ref, x_ref)
    seqs, rows, model = came_ref.shape
    length = x_ref.shape[1] // seqs
    extra = rows - length
    _, held, width = shards_ref.shape
    for i in range(seqs):
        for m in range(model // width):
            which, at = divmod((i * (model // width) + m) * extra, held)
            shards_ref[which, at : at + extra] = came_ref[
                i, length:, m * width : (m + 1) * width
            ]


def arrange_kept(kept, new_query, q_gain, kv_heads):
    seqs, length, model = kept.shape
    hd = q_gain.shape[0]
    heads = new_query.shape[1] // hd
    return pl.pallas_call(
        arrange_kept_kernel,
        out_shape=(
            pltpu.VMEM((2, seqs * length, model // 2), BF16),
            pltpu.VMEM((seqs, heads, kv_heads * hd), BF16),
        ),
        in_specs=[pl.BlockSpec(memory_space=pl.ANY)]
        + [pl.BlockSpec(memory_space=pltpu.VMEM)] * 2,
        scratch_shapes=[pltpu.VMEM(kept.shape, BF16), pltpu.SemaphoreType.DMA],
        compiler_params=vmem(20),
        name="arrange_kept",
    )(*off_chip(kept), new_query, q_gain.reshape(1, hd))


def arrange_came(came, length, shard):
    seqs, _, model = came.shape
    return pl.pallas_call(
        arrange_came_kernel,
        out_shape=(
            pltpu.VMEM((2, seqs * length, model // 2), BF16),
            pltpu.VMEM((2, *shard), BF16),
        ),
        compiler_params=vmem(20),
        name="arrange_came",
    )(came)


def both(refs, core):
    return jnp.concatenate([ref[core] for ref in refs], axis=0)


def two_heads(shard, rows_ref, head):
    parts, hd = rows_ref.shape[1], rows_ref.shape[3]
    rows = shard.shape[0] // parts
    columns = []
    for g in (head, head + 1):
        blocks = []
        for n in range(parts):
            blocks.append(shard[n * rows : (n + 1) * rows, g * hd : (g + 1) * hd])
            blocks.append(rows_ref[g, n])
        columns.append(jnp.concatenate(blocks, axis=0))
    return jnp.concatenate(columns, axis=1)


def partial_kernel(kept_ref, came_ref, shard_ref, rows_ref, out_ref):
    x = both((kept_ref, came_ref), lax.axis_index("c"))
    heads, _, _, hd = rows_ref.shape
    shard = shard_ref[...]
    for g in range(0, heads, 2):
        out_ref[:, g * hd : (g + 2) * hd] = jnp.dot(
            x, two_heads(shard, rows_ref, g), preferred_element_type=F32
        )


def partial_product(x, shard, rows):
    return pl.pallas_call(
        partial_kernel,
        out_shape=pltpu.VMEM((2 * x[0].shape[1], shard.shape[1]), F32),
        compiler_params=vmem(16),
        name="partial",
    )(*on_chip(*x), shard, rows)


def place(ref, seqs, length, g, head):
    core = lax.axis_index("c")
    for n in range(2 * seqs):
        half, i = divmod(n, seqs)
        at = pl.multiple_of((core if half == 0 else 1 - core) * length, 32)
        ref[g * seqs + i, pl.ds(at, length), :] = head[n * length : (n + 1) * length]


def keys_kernel(kept_ref, came_ref, shards_ref, rows_ref, begun_ref, gain_ref, key_ref):
    x = both((kept_ref, came_ref), 1 - lax.axis_index("c"))
    gain = gain_ref[...]
    shard = shards_ref[0]
    kv_heads, hd = rows_ref.shape[0], gain.shape[1]
    seqs = key_ref.shape[0] // kv_heads
    for g in range(0, kv_heads, 2):
        raw = begun_ref[:, g * hd : (g + 2) * hd] + jnp.dot(
            x, two_heads(shard, rows_ref, g), preferred_element_type=F32
        )
        for k in range(2):
            head = root_norm(raw[:, k * hd : (k + 1) * hd], gain).astype(BF16)
            place(key_ref, seqs, key_ref.shape[1] // 2, g + k, head)


def make_keys(x, shards_other, other, begun, gain, seqs):
    kv_heads, hd = other.shape[0], other.shape[3]
    return pl.pallas_call(
        keys_kernel,
        out_shape=pltpu.HBM((kv_heads * seqs, 2 * x[0].shape[1] // seqs, hd), BF16),
        compiler_params=vmem(16),
        name="make_keys",
    )(*on_chip(*x), shards_other, *on_chip(other, begun), gain.reshape(1, hd))


def weigh_kernel(key_ref, query_ref, bias_ref, weight_ref, total_ref):
    seqs, heads, width = query_ref.shape
    hd = key_ref.shape[2]
    span = key_ref.shape[1]
    kv_heads = width // hd
    row = lax.broadcasted_iota(jnp.int32, (heads, 1), 0)
    bias = jnp.zeros((heads, 1), F32)
    for j in range(heads):
        bias = jnp.where(row == j, bias_ref[j], bias)
    scores = []
    for i in range(seqs):
        total = jnp.zeros((heads, span), F32)
        for g in range(kv_heads):
            total += lax.dot_general(
                query_ref[i, :, g * hd : (g + 1) * hd],
                key_ref[g * seqs + i],
                (((1,), (1,)), ((), ())),
                preferred_element_type=F32,
            )
        scores.append(total * (hd**-0.5) + bias)
    scores = jnp.concatenate(scores, axis=0)
    log_keep = -(jnp.maximum(scores, 0.0) + jnp.log1p(jnp.exp(-jnp.abs(scores))))
    first = lax.broadcasted_iota(jnp.int32, (span, span), 0)
    second = lax.broadcasted_iota(jnp.int32, (span, span), 1)
    later = (first > second).astype(BF16)
    after = jnp.zeros(scores.shape, F32)
    rest = log_keep
    for _ in range(3):
        part = rest.astype(BF16)
        rest = rest - part.astype(F32)
        after += jnp.dot(part, later, preferred_element_type=F32)
    weight_high, weight_low = high_low(jnp.exp(scores + log_keep + after))
    total_high, total_low = high_low(jnp.sum(log_keep, axis=1, keepdims=True))
    weight_ref[0], weight_ref[1] = weight_high, weight_low
    total_ref[0] = jnp.broadcast_to(total_high.astype(F32), total_ref.shape[1:])
    total_ref[1] = jnp.broadcast_to(total_low.astype(F32), total_ref.shape[1:])


def weigh(keys, query, bias):
    _, span, hd = keys.shape
    rows = query.shape[0] * query.shape[1]
    here = pl.BlockSpec(memory_space=pltpu.VMEM)
    return pl.pallas_call(
        weigh_kernel,
        out_shape=(pltpu.VMEM((2, rows, span), BF16), pltpu.VMEM((2, rows, hd), F32)),
        in_specs=[here, here, pl.BlockSpec(memory_space=pltpu.SMEM)],
        compiler_params=vmem(8),
        name="weigh",
    )(keys, *on_chip(query), bias)


def values_kernel(
    kept_ref, came_ref, shards_ref, rows_ref, begun_ref, weight_ref, total_ref, value_ref
):
    core = lax.axis_index("c")
    kv_heads, hd = rows_ref.shape[0], rows_ref.shape[3]
    seqs = value_ref.shape[0] // kv_heads
    span = weight_ref.shape[2]
    heads = weight_ref.shape[1] // seqs
    per_group = heads // kv_heads
    x = both((kept_ref, came_ref), 1 - core)
    shard = shards_ref[1]
    weight_high, weight_low = weight_ref[0], weight_ref[1]
    total_high, total_low = total_ref[0], total_ref[1]

    for g in range(0, kv_heads, 2):
        raw = begun_ref[:, g * hd : (g + 2) * hd] + jnp.dot(
            x, two_heads(shard, rows_ref, g), preferred_element_type=F32
        )
        for k in range(2):
            place(value_ref, seqs, span // 2, g + k, raw[:, k * hd : (k + 1) * hd].astype(BF16))

    put = lax.broadcasted_iota(jnp.int32, (EXTRA, 4 * heads), 0)
    take = lax.broadcasted_iota(jnp.int32, (EXTRA, 4 * heads), 1)
    for i in range(seqs):
        at = slice(i * heads, (i + 1) * heads)
        for g in range(kv_heads):
            values = value_ref[g * seqs + i, 0:span]
            read = jnp.dot(weight_high[at], values, preferred_element_type=F32) + jnp.dot(
                weight_low[at], values, preferred_element_type=F32
            )
            read_high, read_low = high_low(read)
            stacked = jnp.concatenate(
                [
                    read_high.astype(F32),
                    read_low.astype(F32),
                    total_high[at],
                    total_low[at],
                ],
                axis=0,
            ).astype(BF16)
            pick = (
                take == (put // per_group) * heads + g * per_group + put % per_group
            ).astype(BF16)
            value_ref[g * seqs + i, span:, :] = jnp.dot(
                pick, stacked, preferred_element_type=F32
            ).astype(BF16)


def make_values(x, shards_other, other, begun, weights, totals):
    _, _, span = weights.shape
    kv_heads, hd = other.shape[0], other.shape[3]
    blocks = kv_heads * x[0].shape[1] * 2 // span
    return pl.pallas_call(
        values_kernel,
        out_shape=pltpu.HBM((blocks, span + EXTRA, hd), BF16),
        compiler_params=vmem(24),
        name="make_values",
    )(*on_chip(*x), shards_other, *on_chip(other, begun, weights, totals))


def store_kernel(rows_ref, out_ref):
    out_ref[...] = rows_ref[...]


def store(rows):
    blocks, span, hd = rows.shape
    spec = pl.BlockSpec((blocks // 4, span, hd), lambda n: (n, 0, 0))
    return pl.pallas_call(
        store_kernel,
        grid=(4,),
        out_shape=pltpu.HBM(rows.shape, rows.dtype),
        in_specs=[spec],
        out_specs=spec,
        compiler_params=vmem(8),
        name="store",
    )(*off_chip(rows))


def join_first_kernel(rows_ref, out_ref):
    count = rows_ref.shape[0]
    shape = (2, rows_ref.shape[2])
    read, log_later = jnp.zeros(shape, F32), jnp.zeros(shape, F32)
    for n in reversed(range(count)):
        rows = rows_ref[n, rows_ref.shape[1] - EXTRA :].astype(F32)
        read += jnp.exp(log_later) * (rows[0:2] + rows[2:4])
        log_later += rows[4:6] + rows[6:8]
    for n in range(out_ref.shape[0]):
        out_ref[n, 0:2] = read
        out_ref[n, 2:4] = log_later


def join_last_kernel(rows_ref, out_ref):
    count = rows_ref.shape[0]
    shape = (2, rows_ref.shape[2])
    read, log_later = jnp.zeros(shape, F32), jnp.zeros(shape, F32)
    for n in reversed(range(count)):
        read += jnp.exp(log_later) * rows_ref[n, 0:2]
        log_later += rows_ref[n, 2:4]
    out_ref[...] = read


def join_first(received, copies):
    return pl.pallas_call(
        join_first_kernel,
        out_shape=jax.ShapeDtypeStruct((copies, 4, received.shape[2]), F32),
        compiler_params=vmem(8),
        name="join_first",
    )(*on_chip(received))


def join_last(pieces):
    return pl.pallas_call(
        join_last_kernel,
        out_shape=jax.ShapeDtypeStruct((2, pieces.shape[2]), F32),
        compiler_params=vmem(4),
        name="join_last",
    )(*on_chip(pieces))


def shards(tokens, in_gain, w_key, w_value, k_gain, new_query, q_gain, stick_bias):
    seq_count, tok_seq, _ = tokens.shape
    head_dim = k_gain.shape[0]
    heads = stick_bias.shape[0]
    kv_heads = w_key.shape[1] // head_dim
    per_group = heads // kv_heads
    seqs = seq_count // 2
    trade = functools.partial(lax.ppermute, axis_name="c", perm=[(0, 1), (1, 0)])
    ys, xs = lax.axis_size("y"), lax.axis_size("x")
    pieces = along_z(w_key, w_value)
    kept, sent = norm_halves(tokens, in_gain, w_key, w_value)
    early, late = spread(pieces, ys * xs)
    came = trade(sent)
    early = lax.all_to_all(early, SP, 0, 0, tiled=True)
    x_kept, query = arrange_kept(kept, new_query, q_gain, kv_heads)
    x_came, shards_other = arrange_came(came, tok_seq, w_key.shape)
    x = (x_kept, x_came)
    early = early.reshape(ys, xs, -1, head_dim)
    early_other = trade(early)
    begun = partial_product(x, w_key, early)
    keys = make_keys(x, shards_other, early_other, begun, k_gain, seqs)
    got_keys = lax.all_to_all(keys, "z", 0, 0, tiled=True)
    late = lax.all_gather(late, SP).reshape(ys, xs, -1, head_dim)
    late_other = trade(late)
    begun = partial_product(x, w_value, late)
    weights, totals = weigh(keys, query, stick_bias)
    values = make_values(x, shards_other, late_other, begun, weights, totals)
    got_values = lax.all_to_all(values, "z", 0, 0, tiled=True)
    stored = store(got_keys)
    joined = join_first(got_values, ys * xs)
    everything = lax.all_to_all(joined, SP, 0, 0, tiled=True)
    read = join_last(everything)
    span = 2 * tok_seq
    positions = got_keys.shape[0] * span
    key_cache = stored.reshape(1, positions, head_dim)
    value_cache = got_values[:, :span].reshape(1, positions, head_dim)
    return (key_cache, value_cache, read.reshape(1, per_group * head_dim))


def solution(mesh):
    grid = Mesh(mesh.devices.reshape(4, 4, 16, 2), ("y", "x", "z", "c"))
    tp = ("z", "c")
    return jax.shard_map(
        shards,
        mesh=grid,
        in_specs=(
            P(None, ("y", "x", "z", "c"), None),
            P(),
            P(tp, None),
            P(tp, None),
            P(),
            P(),
            P(),
            P(),
        ),
        out_specs=(P(tp, SP, None), P(tp, SP, None), P(tp, None)),
        check_vma=False,
    )
```
